128 devices in a mesh: ra: 16 (over z, x), cb: 4 (over y), dp: 2 (over core).
Axes of the slice: x: 4, y: 4, z: 4, core: 2. Of those that a mesh axis runs over, the one named last changes fastest.
Arguments:
- carried: bfloat16 [3072, 4096], P('dp', 'ra'), may hold values from -100 to 100
- branch_in: bfloat16 [3072, 4096], P('dp', 'ra'), may hold values from -12 to 12
- gain_in: float32 [4096], P('ra'), may hold values from 0.1 to 1.9
- bias_in: float32 [4096], P('ra'), may hold values from -1.8 to 1.8
- up_weight: bfloat16 [4096, 16384], P('ra', 'cb'), may hold values from -0.125 to 0.125
- down_weight: bfloat16 [16384, 4096], P('cb', 'ra'), may hold values from -0.046875 to 0.046875
- gain_out: float32 [4096], P('ra'), may hold values from 0.1 to 1.9
- bias_out: float32 [4096], P('ra'), may hold values from -1.8 to 1.8
Outputs:
- layer_out: bfloat16 [3072, 4096], P('dp', 'ra')
The draws below stay inside these ranges and needn't reach their ends.
All inputs are finite; a program needn't handle non-finite values.
Results may differ from the reference program's by a relative error of at most 0.006.
Values may be sent and summed in bfloat16 or wider, within the bound.
A program may use at most 64 MiB of HBM per device.

```python
import math
import jax
import jax.numpy as jnp
from jax import lax

D = 4096
FF = 16384
TOKENS = 3072


def draw_carried(key, part):
    keys = jax.random.split(jax.random.fold_in(key, 11), 3)
    columns = jnp.arange(D, dtype=jnp.float32) / D
    column_scale = 0.5 * 3.0 ** columns * jnp.exp(jax.random.uniform(keys[1], (D,), jnp.float32, -0.5, 0.5))
    values = jnp.clip(jax.random.normal(keys[0], (TOKENS, D), jnp.float32), -4.0, 4.0)
    row_scale = jnp.exp(jax.random.uniform(keys[2], (TOKENS, 1), jnp.float32, 0.0, math.log(10.0)))
    return (values * row_scale * column_scale[None, :]).astype(jnp.bfloat16)


def raised(entries, key, source, target, blocks, factor):
    owner, partner = [(jnp.arange(entries.shape[axis_at]) // (entries.shape[axis_at] // blocks)).reshape([-1 if axis == axis_at else 1 for axis in range(entries.ndim)]) for axis_at in (source, target)]
    chosen = jax.random.permutation(key, blocks)[partner]
    strong = (owner == chosen) | (owner == (partner + blocks // 2) % blocks)
    return jnp.where(strong, factor * entries, entries)


def level_of(stream_key, extent, cuts, least, high):
    level = 1.0
    for position, parts in cuts:
        steps = jax.random.uniform(jax.random.fold_in(jax.random.fold_in(stream_key, 6), position), (parts,), jnp.float32, least / len(cuts), high / len(cuts))
        level = level * jnp.repeat(jnp.exp(steps), extent[position] // parts).reshape((-1,) + (1,) * (len(extent) - 1 - position))
    return level


def noise(stream_key, shape, deviation, limit, cuts=(), held_as=jnp.bfloat16):
    drawn = deviation * jax.random.normal(stream_key, shape, jnp.float32)
    if cuts:
        drawn = drawn * level_of(stream_key, shape, cuts, -0.22, 0.18)
    return jnp.clip(drawn, -limit, limit).astype(held_as)


def heavy_noise(rng, extent, scale, reach, shards, heavy, held_as=jnp.bfloat16):
    array = scale * jax.random.normal(rng, extent, jnp.float32)
    if shards:
        array = array * level_of(rng, extent, shards, -0.22, 0.18)
    return jnp.clip(raised(array, jax.random.fold_in(rng, 3), *heavy), -reach, reach).astype(held_as)


def setup_inputs(seed: int = 0) -> dict:
    seeds = jax.random.split(jax.random.key(seed), 9)
    return {
        "carried": draw_carried(jax.random.fold_in(seeds[8], 71), 0),
        "branch_in": noise(seeds[1], (TOKENS, D), 2.0, 12.0, ((0, 2), (1, 16))),
        "gain_in": jnp.clip(1.0 + 0.18 * jax.random.normal(seeds[2], (D,), jnp.float32), 0.1, 1.9),
        "bias_in": noise(seeds[3], (D,), 0.3, 1.8, ((0, 16),), jnp.float32),
        "up_weight": heavy_noise(seeds[4], (D, FF), D ** -0.5, 0.125, ((0, 16), (1, 4)), (0, 1, 16, 2.0)),
        "down_weight": noise(seeds[5], (FF, D), FF ** -0.5, 0.046875, ((0, 4), (1, 16))),
        "gain_out": jnp.clip(1.0 + 0.18 * jax.random.normal(seeds[6], (D,), jnp.float32), 0.1, 1.9),
        "bias_out": noise(seeds[7], (D,), 0.3, 1.8, ((0, 16),), jnp.float32),
    }


residual_scale = 2.0 ** 0.25
norm_eps = 1e-05

def layer_norm(mixed, gain, bias):
    mean = lax.optimization_barrier(jnp.mean(mixed, axis=-1, keepdims=True))
    spread = lax.optimization_barrier(jnp.mean(mixed * mixed, axis=-1, keepdims=True)) - mean * mean
    return (mixed - mean) * jax.lax.rsqrt(spread + norm_eps) * gain + bias

def reference(carried, branch_in, gain_in, bias_in, up_weight, down_weight, gain_out, bias_out):
    mixed_in = residual_scale * carried.astype(jnp.float32) + branch_in.astype(jnp.float32)
    normed = layer_norm(mixed_in, gain_in, bias_in).astype(jnp.bfloat16)
    pre = jnp.dot(normed, up_weight, preferred_element_type=jnp.float32)
    hidden = jnp.square(jnp.maximum(pre, 0.0)).astype(jnp.bfloat16)
    branch_out = jnp.dot(hidden, down_weight, preferred_element_type=jnp.float32)
    mixed_out = residual_scale * normed.astype(jnp.float32) + branch_out
    return layer_norm(mixed_out, gain_out, bias_out).astype(jnp.bfloat16)
```

```python
import functools

import jax
import jax.numpy as jnp
from jax import lax
from jax.experimental import pallas as pl
from jax.experimental.pallas import tpu as pltpu
from jax.sharding import PartitionSpec as P

residual_scale = 2.0**0.25
norm_eps = 1e-05
MESH = pl.DeviceIdType.MESH
BF = jnp.bfloat16
F32 = jnp.float32

Q = 96
G = 4 * Q
W = 256
D = 16 * W
FS = 1024


def kernel(
    car, bra, gi, bi, wu_in, wd_in, go, bo, out,
    cbuf, bbuf, nloc, nb, wu, wd, hid, pf, pb, opp_p, opp_m, sum_p, sum_m,
    from_m, from_p, rsum, xsend, xrecv, mo, obuf,
    sx_s, sx_r, sz_s, sz_r, tx_s, tx_r, tz_s, tz_r,
    send_sem, recv_sem, local_sem,
):
    r = lax.axis_index("ra")
    y = lax.axis_index("cb")
    c = lax.axis_index("dp")
    z = lax.div(r, 4)
    x = lax.rem(r, 4)

    def turn(i, d):
        return lax.rem(i + d + 4, 4)

    def at_x(d):
        return (z * 4 + turn(x, d), y, c)

    def at_z(d):
        return (turn(z, d) * 4 + x, y, c)

    def at_y(d):
        return (r, turn(y, d), c)

    partner = (r, y, 1 - c)
    remote = []
    local = []

    def send(src, dst, device):
        k = len(remote)
        copy = pltpu.make_async_remote_copy(
            src_ref=src, dst_ref=dst, send_sem=send_sem.at[k], recv_sem=recv_sem.at[k],
            device_id=device, device_id_type=MESH,
        )
        copy.start()
        remote.append(copy)
        return copy

    def fetch(src, dst):
        k = len(local)
        copy = pltpu.make_async_copy(src, dst, local_sem.at[k])
        copy.start()
        local.append(copy)
        return copy

    class Ring:
        def __init__(self, pos, dev, blk):
            self.pos, self.dev, self.blk = pos, dev, blk

        def start(self):
            mine = self.blk(self.pos, None)
            self.p = send(mine, mine, self.dev(1))
            self.m = send(mine, mine, self.dev(-1))

        def forward(self):
            self.p.wait_recv()
            half = self.blk(turn(self.pos, -1), 0)
            self.fp = send(half, half, self.dev(1))
            self.m.wait_recv()
            half = self.blk(turn(self.pos, 1), 1)
            self.fm = send(half, half, self.dev(-1))

        def finish(self):
            self.fp.wait_recv()
            self.fm.wait_recv()

    def rows(start, size, step):
        return pl.ds(pl.multiple_of(start, step), size)

    load_c = fetch(car.at[:, y], cbuf)
    load_b = fetch(bra.at[:, y], bbuf)

    def wrow(zz, xx, cc):
        return (lax.div(zz, 2) * 4 + xx) * 512 + lax.rem(zz, 2) * 256 + cc * 128

    def wblk(zz, xx, half=None):
        start = wrow(zz, xx, c)
        if half is None:
            return wu.at[rows(start, 128, 128), :]
        return wu.at[rows(start + half * 64, 64, 64), :]

    load_wu = fetch(
        wu_in.at[rows(c * 128, 128, 128), rows(x * FS, FS, FS)], wblk(z, x)
    )
    wd_half = rows(c * 512, 512, 512)
    load_wd = fetch(wd_in.at[rows(x * FS + c * 512, 512, 512), :], wd.at[x, wd_half, :])

    barrier = pltpu.get_barrier_semaphore()
    friends = [at_x(1), at_x(2), at_x(3), at_z(1), at_z(2), at_z(3), at_y(1), at_y(3), partner]
    for device in friends:
        pl.semaphore_signal(barrier, inc=1, device_id=device, device_id_type=MESH)

    def mixed_of(i):
        return residual_scale * cbuf[i].astype(F32) + bbuf[i].astype(F32)

    def sums_of(mixed):
        total = jnp.sum(mixed, axis=1, keepdims=True)
        square = jnp.sum(mixed * mixed, axis=1, keepdims=True)
        lane = lax.broadcasted_iota(jnp.int32, (G, 128), 1)
        return jnp.transpose(jnp.where(lane == 0, total, square))[0:8]

    def columns_of(totals):
        row = lax.broadcasted_iota(jnp.int32, (128, G), 0)
        spread = jnp.transpose(jnp.where(row == 0, totals[0:1], totals[1:2]))
        mean = spread[:, 0:1] / D
        var = spread[:, 1:2] / D - mean * mean
        return mean, lax.rsqrt(var + norm_eps)

    def exchange_start(buf, own, got, dev):
        buf[...] = own
        return [send(buf, got.at[d - 1], dev(d)) for d in (1, 2, 3)]

    def exchange_end(copies, buf, got):
        for copy in copies:
            copy.wait_recv()
        return buf[...] + got[0] + got[1] + got[2]

    load_c.wait()
    load_b.wait()
    mixed_in = jnp.concatenate([mixed_of(i) for i in range(4)], axis=0)
    own_sums = sums_of(mixed_in)
    pl.semaphore_wait(barrier, len(friends))

    stat = exchange_start(sx_s, own_sums, sx_r, at_x)
    a2a = {}
    for d in (1, 3, 2):
        to = turn(x, d)
        a2a[d] = send(
            wu_in.at[rows(c * 128, 128, 128), rows(to * FS, FS, FS)], wblk(z, x), at_x(d)
        )
    part = exchange_end(stat, sx_s, sx_r)
    stat = exchange_start(sz_s, part, sz_r, at_z)

    d2d = []

    def share(zz, xx):
        d2d.append(send(wblk(zz, xx), wblk(zz, xx), partner))

    def wring(u):
        xx = turn(x, -u)
        return Ring(z, at_z, lambda i, half: wblk(i, xx, half))

    wrings = {u: wring(u) for u in range(4)}
    load_wu.wait()
    wrings[0].start()
    share(z, x)

    totals = exchange_end(stat, sz_s, sz_r)
    mean, scale = columns_of(totals)
    normed = (
        (jnp.concatenate([mixed_of(i) for i in range(4)], axis=0) - mean) * scale * gi[...]
        + bi[...]
    ).astype(BF)
    for i in range(4):
        nloc[i] = normed[i * Q : (i + 1) * Q]

    ncol = (lax.div(z, 2) * 4 + x) * 512 + lax.rem(z, 2) * 256
    mine = nb.at[rows(y * Q, Q, 32), rows(ncol, W, W)]
    nsend = []
    for d in (1, 3, 2):
        nsend.append(send(nloc.at[turn(z, d)], mine, at_z(d)))
    nb[rows(y * Q, Q, 32), rows(ncol, W, W)] = nloc[z]

    for u in (1, 3):
        a2a[u].wait_recv()
        wrings[u].start()
        share(z, turn(x, -u))

    for copy in nsend:
        copy.wait_recv()

    def ablk1(i, half):
        col, size = (i * 512, 512) if half is None else (i * 512 + half * 256, 256)
        return nb.at[rows(y * Q, Q, 32), rows(col, size, 256)]

    def bblk1(i, half):
        col, size = (2048 + x * 512, 512) if half is None else (2048 + x * 512 + half * 256, 256)
        return nb.at[rows(i * Q, Q, 32), rows(col, size, 256)]

    def ablk2(i, half):
        cols = pl.ds(0, 2048) if half is None else pl.ds(half * 1024, 1024)
        return nb.at[rows(i * Q, Q, 32), cols]

    def bblk2(i, half):
        col, size = (2048 + i * 512, 512) if half is None else (2048 + i * 512 + half * 256, 256)
        return nb.at[:, rows(col, size, 256)]

    a1, b1 = Ring(x, at_x, ablk1), Ring(y, at_y, bblk1)
    a2, b2 = Ring(y, at_y, ablk2), Ring(x, at_x, bblk2)
    a1.start()
    b1.start()
    a2a[2].wait_recv()
    wrings[2].start()
    share(z, turn(x, -2))
    b1.forward()
    a1.forward()
    b1.finish()
    b2.start()
    a1.finish()
    a2.start()

    wd_a2a = []
    for d in (1, 3, 2):
        to = turn(x, d)
        wd_a2a.append(
            send(wd_in.at[rows(to * FS + c * 512, 512, 512), :], wd.at[x, wd_half, :], at_x(d))
        )

    for u in (0, 1, 3, 2):
        wrings[u].forward()
        share(turn(z, -1), turn(x, -u))
        share(turn(z, 1), turn(x, -u))
    b2.forward()
    a2.forward()
    for u in (0, 1, 3, 2):
        wrings[u].finish()
        share(turn(z, 2), turn(x, -u))
    load_wd.wait()
    wshare = [send(wd.at[x, wd_half, :], wd.at[x, wd_half, :], partner)]
    for copy, d in zip(wd_a2a, (1, 3, 2)):
        copy.wait_recv()
        at = wd.at[turn(x, -d), wd_half, :]
        wshare.append(send(at, at, partner))
    b2.finish()
    a2.finish()
    for copy in d2d:
        copy.wait_recv()

    hrings = []
    for n in range(4):
        cols = slice(n * 256, (n + 1) * 256)
        pre = jnp.dot(nb[...], wu[:, cols], preferred_element_type=F32)
        hid[z, :, cols] = jnp.square(jnp.maximum(pre, 0.0)).astype(BF)

        def hblk(i, half, n=n):
            if half is None:
                return hid.at[i, :, pl.ds(n * 256, 256)]
            return hid.at[i, pl.ds(half * 192, 192), pl.ds(n * 256, 256)]

        hrings.append(Ring(z, at_z, hblk))
        hrings[n].start()
    for copy in wshare:
        copy.wait_recv()

    def down(k, group):
        for j in range(4):
            part = jnp.dot(hid[group], wd[j], preferred_element_type=F32)
            pf[k, j] = part
            pb[k, j] = part.astype(BF)

    yp, ym = turn(y, 1), turn(y, -1)

    def quarter(ref, k, q, half):
        return ref.at[k, pl.ds(half * 2, 2), rows(q * Q, Q, 32), :]

    state = {}

    def y_first(k):
        q = turn(y, 2)
        s = {}
        s["op"] = send(quarter(pb, k, q, 0), opp_p.at[k], at_y(1))
        s["om"] = send(quarter(pb, k, q, 1), opp_m.at[k], at_y(-1))
        s["dp"] = send(quarter(pb, k, yp, 1), from_m.at[k, pl.ds(2, 2)], at_y(1))
        s["dm"] = send(quarter(pb, k, ym, 0), from_p.at[k, pl.ds(0, 2)], at_y(-1))
        state[k] = s

    def y_second(k):
        s = state[k]
        s["op"].wait_recv()
        sum_p[k] = (pf[k, 0:2, rows(yp * Q, Q, 32), :] + opp_p[k].astype(F32)).astype(BF)
        s["sp"] = send(sum_p.at[k], from_m.at[k, pl.ds(0, 2)], at_y(1))
        s["om"].wait_recv()
        sum_m[k] = (pf[k, 2:4, rows(ym * Q, Q, 32), :] + opp_m[k].astype(F32)).astype(BF)
        s["sm"] = send(sum_m.at[k], from_p.at[k, pl.ds(2, 2)], at_y(-1))

    def x_first(k):
        s = state[k]
        for name in ("dp", "dm", "sp", "sm"):
            s[name].wait_recv()
        total = (
            pf[k, :, rows(y * Q, Q, 32), :] + from_m[k].astype(F32) + from_p[k].astype(F32)
        )
        rsum[k] = total
        xsend[k] = total.astype(BF)
        s["x"] = [send(xsend.at[k, turn(x, d)], xrecv.at[k, d - 1], at_x(d)) for d in (1, 3, 2)]

    def x_second(k, group):
        for copy in state[k]["x"]:
            copy.wait_recv()
        branch = rsum[k, x]
        for d in range(3):
            branch = branch + xrecv[k, d].astype(F32)
        mo[group] = residual_scale * nloc[group].astype(F32) + branch

    groups = [z, turn(z, -1), turn(z, 1), turn(z, 2)]
    down(0, groups[0])
    y_first(0)
    for ring in hrings:
        ring.forward()
    y_second(0)
    down(1, groups[1])
    y_first(1)
    down(2, groups[2])
    y_first(2)
    x_first(0)
    y_second(1)
    y_second(2)
    for ring in hrings:
        ring.finish()
    down(3, groups[3])
    y_first(3)
    x_first(1)
    x_first(2)
    x_second(0, groups[0])
    y_second(3)
    x_second(1, groups[1])
    x_second(2, groups[2])
    x_first(3)
    x_second(3, groups[3])

    mixed_out = jnp.concatenate([mo[i] for i in range(4)], axis=0)
    stat = exchange_start(tx_s, sums_of(mixed_out), tx_r, at_x)
    part = exchange_end(stat, tx_s, tx_r)
    stat = exchange_start(tz_s, part, tz_r, at_z)
    totals = exchange_end(stat, tz_s, tz_r)
    mean, scale = columns_of(totals)
    mixed_out = jnp.concatenate([mo[i] for i in range(4)], axis=0)
    result = ((mixed_out - mean) * scale * go[...] + bo[...]).astype(BF)
    for i in range(4):
        obuf[y, i] = result[i * Q : (i + 1) * Q]

    def oblk(i, half):
        if half is None:
            return obuf.at[i]
        return obuf.at[i, pl.ds(half * 2, 2)]

    ring = Ring(y, at_y, oblk)
    ring.start()
    stores = [fetch(obuf.at[y], out.at[:, y])]
    ring.forward()
    stores.append(fetch(obuf.at[ym], out.at[:, ym]))
    stores.append(fetch(obuf.at[yp], out.at[:, yp]))
    ring.finish()
    far = turn(y, 2)
    stores.append(fetch(obuf.at[far], out.at[:, far]))
    assert len(remote) == N_REMOTE and len(local) == N_LOCAL
    for copy in remote:
        copy.wait_send()
    for copy in stores:
        copy.wait()


N_REMOTE = 129
N_LOCAL = 8


def per_device(carried, branch_in, gain_in, bias_in, up_weight, down_weight, gain_out, bias_out):
    any_spec = pl.BlockSpec(memory_space=pl.ANY)
    vmem_spec = pl.BlockSpec(memory_space=pltpu.VMEM)
    V = pltpu.VMEM
    result = pl.pallas_call(
        kernel,
        out_shape=jax.ShapeDtypeStruct((4, 4, Q, W), BF),
        in_specs=[any_spec, any_spec, vmem_spec, vmem_spec, any_spec, any_spec, vmem_spec, vmem_spec],
        out_specs=any_spec,
        scratch_shapes=[
            V((4, Q, W), BF), V((4, Q, W), BF), V((4, Q, W), BF),
            V((G, D), BF), V((D, FS), BF), V((4, FS, W), BF), V((4, G, FS), BF),
            V((4, 4, G, W), F32), V((4, 4, G, W), BF),
            V((4, 2, Q, W), BF), V((4, 2, Q, W), BF), V((4, 2, Q, W), BF), V((4, 2, Q, W), BF),
            V((4, 4, Q, W), BF), V((4, 4, Q, W), BF),
            V((4, 4, Q, W), F32), V((4, 4, Q, W), BF), V((4, 3, Q, W), BF),
            V((4, Q, W), F32), V((4, 4, Q, W), BF),
            V((8, G), F32), V((3, 8, G), F32), V((8, G), F32), V((3, 8, G), F32),
            V((8, G), F32), V((3, 8, G), F32), V((8, G), F32), V((3, 8, G), F32),
            pltpu.SemaphoreType.DMA((N_REMOTE,)),
            pltpu.SemaphoreType.DMA((N_REMOTE,)),
            pltpu.SemaphoreType.DMA((N_LOCAL,)),
        ],
        compiler_params=pltpu.CompilerParams(
            collective_id=0, has_side_effects=True, vmem_limit_bytes=60 * 1024 * 1024
        ),
    )(
        carried.reshape(4, 4, Q, W), branch_in.reshape(4, 4, Q, W),
        gain_in.reshape(1, W), bias_in.reshape(1, W), up_weight, down_weight,
        gain_out.reshape(1, W), bias_out.reshape(1, W),
    )
    return result.reshape(carried.shape)


def solution(mesh):
    in_specs = (
        P("dp", "ra"),
        P("dp", "ra"),
        P("ra"),
        P("ra"),
        P("ra", "cb"),
        P("cb", "ra"),
        P("ra"),
        P("ra"),
    )
    out_specs = P("dp", "ra")
    return jax.shard_map(
        per_device, mesh=mesh, in_specs=in_specs, out_specs=out_specs, check_vma=False
    )
```

```python
import functools

import jax
import jax.numpy as jnp
from jax import lax
from jax.experimental import pallas as pl
from jax.experimental.pallas import tpu as pltpu
from jax.sharding import PartitionSpec as P

residual_scale = 2.0**0.25
norm_eps = 1e-05
MESH = pl.DeviceIdType.MESH
BF = jnp.bfloat16
F32 = jnp.float32

Q = 96
G = 4 * Q
W = 256
D = 16 * W
FS = 1024


def kernel(
    car, bra, gi, bi, wu_in, wd_in, go, bo, out,
    cbuf, bbuf, nloc, nb, wu, wd, hid, pf, pb, opp_p, opp_m, sum_p, sum_m,
    from_m, from_p, rsum, tosend, torecv, mo, mob, obuf,
    sx_s, sx_r, sz_s, sz_r, tx_s, tx_r, tz_s, tz_r, totals, means, scales,
    send_sem, recv_sem, local_sem,
):
    r = lax.axis_index("ra")
    y = lax.axis_index("cb")
    c = lax.axis_index("dp")
    z = lax.div(r, 4)
    x = lax.rem(r, 4)

    def turn(i, d):
        return lax.rem(i + d + 4, 4)

    def at_x(d):
        return (z * 4 + turn(x, d), y, c)

    def at_z(d):
        return (turn(z, d) * 4 + x, y, c)

    def at_y(d):
        return (r, turn(y, d), c)

    partner = (r, y, 1 - c)
    remote = []
    local = []

    def send(src, dst, device):
        k = len(remote)
        copy = pltpu.make_async_remote_copy(
            src_ref=src, dst_ref=dst, send_sem=send_sem.at[k], recv_sem=recv_sem.at[k],
            device_id=device, device_id_type=MESH,
        )
        copy.start()
        remote.append(copy)
        return copy

    def fetch(src, dst):
        k = len(local)
        copy = pltpu.make_async_copy(src, dst, local_sem.at[k])
        copy.start()
        local.append(copy)
        return copy

    class Ring:
        def __init__(self, pos, dev, blk):
            self.pos, self.dev, self.blk = pos, dev, blk

        def start(self):
            mine = self.blk(self.pos, None)
            self.p = send(mine, mine, self.dev(1))
            self.m = send(mine, mine, self.dev(-1))

        def forward(self):
            self.p.wait_recv()
            half = self.blk(turn(self.pos, -1), 0)
            self.fp = send(half, half, self.dev(1))
            self.m.wait_recv()
            half = self.blk(turn(self.pos, 1), 1)
            self.fm = send(half, half, self.dev(-1))

        def finish(self):
            self.fp.wait_recv()
            self.fm.wait_recv()

    def rows(start, size, step):
        return pl.ds(pl.multiple_of(start, step), size)

    load_c = fetch(car.at[:, y], cbuf)
    load_b = fetch(bra.at[:, y], bbuf)

    def wrow(zz, xx, cc):
        return (lax.div(zz, 2) * 4 + xx) * 512 + lax.rem(zz, 2) * 256 + cc * 128

    def wblk(zz, xx, f, half=None):
        start = wrow(zz, xx, c)
        if half is None:
            return wu.at[rows(start, 128, 128), pl.ds(f * 512, 512)]
        return wu.at[rows(start + half * 64, 64, 64), pl.ds(f * 512, 512)]

    load_wu = fetch(
        wu_in.at[rows(c * 128, 128, 128), rows(x * FS, FS, FS)],
        wu.at[rows(wrow(z, x, c), 128, 128), :],
    )
    wd_half = rows(c * 512, 512, 512)
    load_wd = fetch(wd_in.at[rows(x * FS + c * 512, 512, 512), :], wd.at[x, wd_half, :])

    barrier = pltpu.get_barrier_semaphore()
    friends = [dev(d) for dev in (at_x, at_z, at_y) for d in (1, 2, 3)] + [partner]
    for device in friends:
        pl.semaphore_signal(barrier, inc=1, device_id=device, device_id_type=MESH)

    def mixed_of(i):
        return residual_scale * cbuf[i].astype(F32) + bbuf[i].astype(F32)

    def sums_of(mixed):
        total = jnp.sum(mixed, axis=1, keepdims=True)
        square = jnp.sum(mixed * mixed, axis=1, keepdims=True)
        lane = lax.broadcasted_iota(jnp.int32, (mixed.shape[0], 128), 1)
        return jnp.transpose(jnp.where(lane == 0, total, square))[0:8]

    def columns_of(sums):
        row = lax.broadcasted_iota(jnp.int32, (128, sums.shape[1]), 0)
        spread = jnp.transpose(jnp.where(row == 0, sums[0:1], sums[1:2]))
        mean = spread[:, 0:1] / D
        var = spread[:, 1:2] / D - mean * mean
        return mean, lax.rsqrt(var + norm_eps)

    def exchange_start(buf, own, got, dev):
        buf[...] = own
        return [send(buf, got.at[d - 1], dev(d)) for d in (1, 2, 3)]

    def exchange_end(copies, buf, got):
        for copy in copies:
            copy.wait_recv()
        return buf[...] + got[0] + got[1] + got[2]

    d2d = {0: [], 1: []}

    def share(zz, xx, f):
        d2d[f].append(send(wblk(zz, xx, f), wblk(zz, xx, f), partner))

    def wring(u, f):
        xx = turn(x, -u)
        return Ring(z, at_z, lambda i, half: wblk(i, xx, f, half))

    wrings = {(u, f): wring(u, f) for u in range(4) for f in range(2)}
    a2a = {}

    def wu_send(d, f):
        cols = rows(turn(x, d) * FS + f * 512, 512, 512)
        a2a[d, f] = send(wu_in.at[rows(c * 128, 128, 128), cols], wblk(z, x, f), at_x(d))

    def w_start(u, f):
        if u:
            a2a[u, f].wait_recv()
        wrings[u, f].start()
        share(z, turn(x, -u), f)

    def w_forward(u, f):
        wrings[u, f].forward()
        share(turn(z, -1), turn(x, -u), f)
        share(turn(z, 1), turn(x, -u), f)

    def w_finish(u, f):
        wrings[u, f].finish()
        share(turn(z, 2), turn(x, -u), f)

    load_c.wait()
    load_b.wait()
    mixed_in = jnp.concatenate([mixed_of(i) for i in range(4)], axis=0)
    own_sums = sums_of(mixed_in)
    load_wu.wait()
    pl.semaphore_wait(barrier, len(friends))

    stat = exchange_start(sx_s, own_sums, sx_r, at_x)
    w_start(0, 0)
    for d in (1, 3, 2):
        wu_send(d, 0)
    w_start(0, 1)
    wu_send(1, 1)
    wu_send(3, 1)
    part = exchange_end(stat, sx_s, sx_r)
    stat = exchange_start(sz_s, part, sz_r, at_z)
    w_start(1, 0)
    mean, scale = columns_of(exchange_end(stat, sz_s, sz_r))
    normed = (
        (jnp.concatenate([mixed_of(i) for i in range(4)], axis=0) - mean) * scale * gi[...]
        + bi[...]
    ).astype(BF)
    for i in range(4):
        nloc[i] = normed[i * Q : (i + 1) * Q]

    ncol = (lax.div(z, 2) * 4 + x) * 512 + lax.rem(z, 2) * 256
    mine = nb.at[rows(y * Q, Q, 32), rows(ncol, W, W)]
    nsend = []
    for d in (1, 3, 2):
        nsend.append(send(nloc.at[turn(z, d)], mine, at_z(d)))
    nb[rows(y * Q, Q, 32), rows(ncol, W, W)] = nloc[z]
    w_start(3, 0)
    w_forward(0, 0)
    for copy in nsend:
        copy.wait_recv()

    def nblk(h, xx, yy, part):
        col, size = h * 2048 + xx * 512, 512
        if part is not None:
            col, size = col + part * 256, 256
        return nb.at[rows(yy * Q, Q, 32), rows(col, size, 256)]

    a1 = Ring(x, at_x, lambda i, part: nblk(0, i, y, part))
    b1 = Ring(y, at_y, lambda i, part: nblk(1, x, i, part))

    def second(j):
        return (
            Ring(y, at_y, lambda i, part: nblk(0, turn(x, -j), i, part)),
            Ring(x, at_x, lambda i, part: nblk(1, i, turn(y, -j), part)),
        )

    seconds = [second(j) for j in range(4)]

    def n_start(j):
        for ring in seconds[j]:
            ring.start()

    def n_forward(j):
        for ring in seconds[j]:
            ring.forward()

    a1.start()
    b1.start()
    n_start(0)
    w_start(2, 0)
    w_forward(1, 0)
    b1.forward()
    a1.forward()
    n_start(1)
    n_start(3)
    wu_send(2, 1)
    w_start(1, 1)
    w_forward(3, 0)
    w_forward(0, 1)
    n_forward(0)
    b1.finish()
    a1.finish()
    n_start(2)
    w_start(3, 1)
    w_forward(2, 0)
    for u in (0, 1, 3):
        w_finish(u, 0)
    n_forward(1)
    w_forward(1, 1)
    w_start(2, 1)
    w_finish(2, 0)
    w_finish(0, 1)
    n_forward(3)
    w_forward(3, 1)
    n_forward(2)

    wd_a2a = []
    for d in (1, 3, 2):
        to = turn(x, d)
        wd_a2a.append(
            send(wd_in.at[rows(to * FS + c * 512, 512, 512), :], wd.at[x, wd_half, :], at_x(d))
        )
    load_wd.wait()
    wshare = [send(wd.at[x, wd_half, :], wd.at[x, wd_half, :], partner)]
    w_forward(2, 1)
    for pair in seconds:
        for ring in pair:
            ring.finish()
    for copy in d2d[0]:
        copy.wait_recv()

    hrings = []

    def up(n):
        cols = slice(n * 256, (n + 1) * 256)
        pre = jnp.dot(nb[...], wu[:, cols], preferred_element_type=F32)
        hid[z, :, cols] = jnp.square(jnp.maximum(pre, 0.0)).astype(BF)

        def hblk(i, half):
            if half is None:
                return hid.at[i, :, pl.ds(n * 256, 256)]
            return hid.at[i, pl.ds(half * 192, 192), pl.ds(n * 256, 256)]

        ring = Ring(z, at_z, hblk)
        ring.start()
        hrings.append(ring)

    up(0)
    for u in (1, 3, 2):
        w_finish(u, 1)
    up(1)
    for copy, d in zip(wd_a2a, (1, 3, 2)):
        copy.wait_recv()
        at = wd.at[turn(x, -d), wd_half, :]
        wshare.append(send(at, at, partner))
    for copy in d2d[1]:
        copy.wait_recv()
    up(2)
    up(3)
    for copy in wshare:
        copy.wait_recv()

    def down(k, group):
        for j in range(4):
            part = jnp.dot(hid[group], wd[j], preferred_element_type=F32)
            for i in range(4):
                pf[k, j, i] = part[i * Q : (i + 1) * Q]
                pb[k, j, i] = part[i * Q : (i + 1) * Q].astype(BF)

    class Reduce:
        def __init__(self, k, kind):
            self.at = (k, kind)
            self.k = k
            self.kind = kind
            self.pos, self.dev = ((y, at_y), (x, at_x))[kind]
            self.pos2, self.dev2 = ((x, at_x), (y, at_y))[kind]

        def item(self, to, first, count):
            if self.kind == 0:
                return (self.k, pl.ds(first, count), to, pl.ds(0, 48), slice(None))
            return (self.k, to, pl.ds(first, count), pl.ds(48, 48), slice(None))

        def first(self):
            far, p, m = turn(self.pos, 2), turn(self.pos, 1), turn(self.pos, -1)
            self.p, self.m = p, m
            self.op = send(pb.at[self.item(far, 0, 2)], opp_p.at[self.at], self.dev(1))
            self.om = send(pb.at[self.item(far, 2, 2)], opp_m.at[self.at], self.dev(-1))
            low, high = pl.ds(0, 2), pl.ds(2, 2)
            self.dp = send(
                pb.at[self.item(p, 2, 2)], from_m.at[(*self.at, high)], self.dev(1)
            )
            self.dm = send(
                pb.at[self.item(m, 0, 2)], from_p.at[(*self.at, low)], self.dev(-1)
            )

        def second(self):
            low, high = pl.ds(0, 2), pl.ds(2, 2)
            self.op.wait_recv()
            sum_p[self.at] = (pf[self.item(self.p, 0, 2)] + opp_p[self.at].astype(F32)).astype(BF)
            self.sp = send(sum_p.at[self.at], from_m.at[(*self.at, low)], self.dev(1))
            self.om.wait_recv()
            sum_m[self.at] = (pf[self.item(self.m, 2, 2)] + opp_m[self.at].astype(F32)).astype(BF)
            self.sm = send(sum_m.at[self.at], from_p.at[(*self.at, high)], self.dev(-1))

        def third(self):
            for copy in (self.dp, self.dm, self.sp, self.sm):
                copy.wait_recv()
            total = (
                pf[self.item(self.pos, 0, 4)]
                + from_m[self.at].astype(F32)
                + from_p[self.at].astype(F32)
            )
            rsum[self.at] = total
            tosend[self.at] = total.astype(BF)
            self.last = [
                send(
                    tosend.at[(*self.at, turn(self.pos2, d))],
                    torecv.at[(*self.at, d - 1)],
                    self.dev2(d),
                )
                for d in (1, 3, 2)
            ]

        def fourth(self, group):
            for copy in self.last:
                copy.wait_recv()
            branch = rsum[(*self.at, self.pos2)]
            for d in range(3):
                branch = branch + torecv[(*self.at, d)].astype(F32)
            part = slice(self.kind * 48, self.kind * 48 + 48)
            mixed = residual_scale * nloc[group, part].astype(F32) + branch
            mo[group, part] = mixed
            mob[y, self.k, part] = mixed.astype(BF)

    groups = [z, turn(z, -1), turn(z, 1), turn(z, 2)]
    reduces = [(Reduce(k, 0), Reduce(k, 1)) for k in range(4)]

    def first(k):
        down(k, groups[k])
        for one in reduces[k]:
            one.first()

    def second_(k):
        for one in reduces[k]:
            one.second()

    def third(k):
        for one in reduces[k]:
            one.third()

    def fourth(k):
        for one in reduces[k]:
            one.fourth(groups[k])

    first(0)
    hrings[0].forward()
    hrings[1].forward()
    second_(0)
    hrings[2].forward()
    third(0)
    hrings[3].forward()
    first(1)
    first(2)
    fourth(0)
    second_(1)
    second_(2)
    third(1)
    third(2)
    for ring in hrings:
        ring.finish()
    first(3)
    fourth(1)
    fourth(2)

    def mblk(i, half):
        if half is None:
            return mob.at[i, pl.ds(0, 3)]
        return mob.at[i, pl.ds(0, 3), pl.ds(half * 48, 48)]

    ring = Ring(y, at_y, mblk)
    ring.start()
    second_(3)
    third(3)
    ring.forward()
    fourth(3)
    mixed_out = jnp.concatenate([mo[i] for i in range(4)], axis=0)
    stat = exchange_start(tx_s, sums_of(mixed_out), tx_r, at_x)
    last = [send(mob.at[y, 3], mob.at[y, 3], at_y(d)) for d in (1, 3, 2)]
    part = exchange_end(stat, tx_s, tx_r)
    stat = exchange_start(tz_s, part, tz_r, at_z)
    ring.finish()
    for copy in last:
        copy.wait_recv()
    totals[y] = exchange_end(stat, tz_s, tz_r)
    stat = [send(totals.at[y], totals.at[y], at_y(d)) for d in (1, 3, 2)]
    stores = []

    def finish(yy):
        mean, scale = columns_of(totals[yy])
        for i in range(4):
            means[i] = jnp.broadcast_to(mean[i * Q : (i + 1) * Q], (Q, 128))
            scales[i] = jnp.broadcast_to(scale[i * Q : (i + 1) * Q], (Q, 128))
        for k in range(4):
            mean = means[groups[k]][:, 0:1]
            scale = scales[groups[k]][:, 0:1]
            block = (mob[yy, k].astype(F32) - mean) * scale * go[...] + bo[...]
            obuf[yy, k] = block.astype(BF)
            stores.append(fetch(obuf.at[yy, k], out.at[groups[k], yy]))

    finish(y)
    for copy, d in zip(stat, (1, 3, 2)):
        copy.wait_recv()
        finish(turn(y, -d))
    assert (len(remote), len(local)) == (N_REMOTE, N_LOCAL), (len(remote), len(local))
    for copy in remote:
        copy.wait_send()
    for copy in stores:
        copy.wait()


N_REMOTE = 230
N_LOCAL = 20


def per_device(carried, branch_in, gain_in, bias_in, up_weight, down_weight, gain_out, bias_out):
    any_spec = pl.BlockSpec(memory_space=pl.ANY)
    vmem_spec = pl.BlockSpec(memory_space=pltpu.VMEM)
    V = pltpu.VMEM
    result = pl.pallas_call(
        kernel,
        out_shape=jax.ShapeDtypeStruct((4, 4, Q, W), BF),
        in_specs=[any_spec, any_spec, vmem_spec, vmem_spec, any_spec, any_spec, vmem_spec, vmem_spec],
        out_specs=any_spec,
        scratch_shapes=[
            V((4, Q, W), BF), V((4, Q, W), BF), V((4, Q, W), BF),
            V((G, D), BF), V((D, FS), BF), V((4, FS, W), BF), V((4, G, FS), BF),
            V((4, 4, 4, Q, W), F32), V((4, 4, 4, Q, W), BF),
            *[V((4, 2, 2, 48, W), BF) for _ in range(4)],
            V((4, 2, 4, 48, W), BF), V((4, 2, 4, 48, W), BF),
            V((4, 2, 4, 48, W), F32), V((4, 2, 4, 48, W), BF), V((4, 2, 3, 48, W), BF),
            V((4, Q, W), F32), V((4, 4, Q, W), BF), V((4, 4, Q, W), BF),
            *[V(shape, F32) for shape in ((8, G), (3, 8, G)) * 4],
            V((4, 8, G), F32), V((4, Q, 128), F32), V((4, Q, 128), F32),
            pltpu.SemaphoreType.DMA((N_REMOTE,)),
            pltpu.SemaphoreType.DMA((N_REMOTE,)),
            pltpu.SemaphoreType.DMA((N_LOCAL,)),
        ],
        compiler_params=pltpu.CompilerParams(
            collective_id=0, has_side_effects=True, vmem_limit_bytes=60 * 1024 * 1024
        ),
    )(
        carried.reshape(4, 4, Q, W), branch_in.reshape(4, 4, Q, W),
        gain_in.reshape(1, W), bias_in.reshape(1, W), up_weight, down_weight,
        gain_out.reshape(1, W), bias_out.reshape(1, W),
    )
    return result.reshape(carried.shape)


def solution(mesh):
    in_specs = (
        P("dp", "ra"),
        P("dp", "ra"),
        P("ra"),
        P("ra"),
        P("ra", "cb"),
        P("cb", "ra"),
        P("ra"),
        P("ra"),
    )
    out_specs = P("dp", "ra")
    return jax.shard_map(
        per_device, mesh=mesh, in_specs=in_specs, out_specs=out_specs, check_vma=False
    )
```

```python
import functools

import jax
import jax.numpy as jnp
from jax import lax
from jax.experimental import pallas as pl
from jax.experimental.pallas import tpu as pltpu
from jax.sharding import PartitionSpec as P

residual_scale = 2.0**0.25
norm_eps = 1e-05
MESH = pl.DeviceIdType.MESH
BF = jnp.bfloat16
F32 = jnp.float32

Q = 96
G = 4 * Q
W = 256
D = 16 * W
FS = 1024


def kernel(
    car, bra, gi, bi, wu_in, wd_in, go, bo, out,
    cbuf, bbuf, nloc, nb, wu, wd, hid, pf, pb, opp_p, opp_m, sum_p, sum_m,
    from_m, from_p, rsum, tosend, torecv, mo, mob, obuf,
    sx_s, sx_r, sz_s, sz_r, tx_s, tx_r, tz_s, tz_r, totals,
    send_sem, recv_sem, local_sem,
):
    r = lax.axis_index("ra")
    y = lax.axis_index("cb")
    c = lax.axis_index("dp")
    z = lax.div(r, 4)
    x = lax.rem(r, 4)

    def turn(i, d):
        return lax.rem(i + d + 4, 4)

    def at_x(d):
        return (z * 4 + turn(x, d), y, c)

    def at_z(d):
        return (turn(z, d) * 4 + x, y, c)

    def at_y(d):
        return (r, turn(y, d), c)

    partner = (r, y, 1 - c)
    remote = []
    local = []

    used = []

    def channel():
        used.append(len(used))
        return used[-1]

    def described(src, dst, device, slot, on):
        return pltpu.make_async_remote_copy(
            src_ref=src, dst_ref=dst, send_sem=send_sem.at[slot], recv_sem=recv_sem.at[on],
            device_id=device, device_id_type=MESH,
        )

    def send(src, dst, device, on=None):
        k = len(remote)
        if k >= N_SEND:
            remote[k - N_SEND].wait_send()
        copy = described(src, dst, device, k % N_SEND, channel() if on is None else on)
        copy.start()
        remote.append(copy)
        return copy

    def expect(on, cover):
        described(cover, cover, partner, 0, on).wait_recv()

    def fetch(src, dst, on=None):
        k = len(local) if on is None else on
        copy = pltpu.make_async_copy(src, dst, local_sem.at[k])
        copy.start()
        local.append(copy)
        return copy

    class Ring:
        def __init__(self, pos, dev, blk):
            self.pos, self.dev, self.blk = pos, dev, blk

        def start(self):
            mine = self.blk(self.pos, None)
            self.p = send(mine, mine, self.dev(1))
            self.m = send(mine, mine, self.dev(-1))

        def forward(self):
            self.on = channel()
            self.p.wait_recv()
            half = self.blk(turn(self.pos, -1), 0)
            send(half, half, self.dev(1), self.on)
            self.m.wait_recv()
            half = self.blk(turn(self.pos, 1), 1)
            send(half, half, self.dev(-1), self.on)

        def finish(self):
            expect(self.on, self.blk(turn(self.pos, 2), None))

    def rows(start, size, step):
        return pl.ds(pl.multiple_of(start, step), size)

    load_c = fetch(car.at[:, y], cbuf)
    load_b = fetch(bra.at[:, y], bbuf)

    def wrow(zz, xx, cc):
        return (lax.div(zz, 2) * 4 + xx) * 512 + lax.rem(zz, 2) * 256 + cc * 128

    def wblk(zz, xx, f, half=None):
        start = wrow(zz, xx, c)
        if half is None:
            return wu.at[rows(start, 128, 128), pl.ds(f * 512, 512)]
        return wu.at[rows(start + half * 64, 64, 64), pl.ds(f * 512, 512)]

    load_wu = fetch(
        wu_in.at[rows(c * 128, 128, 128), rows(x * FS, FS, FS)],
        wu.at[rows(wrow(z, x, c), 128, 128), :],
    )
    wd_half = rows(c * 512, 512, 512)
    load_wd = fetch(wd_in.at[rows(x * FS + c * 512, 512, 512), :], wd.at[x, wd_half, :])

    barrier = pltpu.get_barrier_semaphore()
    friends = [dev(d) for dev in (at_x, at_z, at_y) for d in (1, 2, 3)] + [partner]
    for device in friends:
        pl.semaphore_signal(barrier, inc=1, device_id=device, device_id_type=MESH)

    def mixed_of(i):
        return residual_scale * cbuf[i].astype(F32) + bbuf[i].astype(F32)

    def sums_of(mixed):
        total = jnp.sum(mixed, axis=1, keepdims=True)
        square = jnp.sum(mixed * mixed, axis=1, keepdims=True)
        lane = lax.broadcasted_iota(jnp.int32, (mixed.shape[0], 128), 1)
        return jnp.transpose(jnp.where(lane == 0, total, square))[0:8]

    def columns_of(sums):
        row = lax.broadcasted_iota(jnp.int32, (128, sums.shape[1]), 0)
        spread = jnp.transpose(jnp.where(row == 0, sums[0:1], sums[1:2]))
        mean = spread[:, 0:1] / D
        var = spread[:, 1:2] / D - mean * mean
        return mean, lax.rsqrt(var + norm_eps)

    def exchange_start(buf, own, got, dev):
        buf[...] = own
        on = channel()
        for d in (1, 2, 3):
            send(buf, got.at[d - 1], dev(d), on)
        return on

    def exchange_end(on, buf, got):
        expect(on, got)
        return buf[...] + got[0] + got[1] + got[2]

    d2d = (channel(), channel())

    def share(zz, xx, f):
        send(wblk(zz, xx, f), wblk(zz, xx, f), partner, d2d[f])

    def shared(f):
        expect(d2d[f], wu.at[pl.ds(0, D // 2), pl.ds(f * 512, 512)])

    def wring(u, f):
        xx = turn(x, -u)
        return Ring(z, at_z, lambda i, half: wblk(i, xx, f, half))

    wrings = {(u, f): wring(u, f) for u in range(4) for f in range(2)}
    a2a = {}

    def wu_send(d, f):
        cols = rows(turn(x, d) * FS + f * 512, 512, 512)
        a2a[d, f] = send(wu_in.at[rows(c * 128, 128, 128), cols], wblk(z, x, f), at_x(d))

    def w_start(u, f):
        if u:
            a2a[u, f].wait_recv()
        wrings[u, f].start()
        share(z, turn(x, -u), f)

    def w_forward(u, f):
        wrings[u, f].forward()
        share(turn(z, -1), turn(x, -u), f)
        share(turn(z, 1), turn(x, -u), f)

    def w_finish(u, f):
        wrings[u, f].finish()
        share(turn(z, 2), turn(x, -u), f)

    load_c.wait()
    load_b.wait()
    mixed_in = jnp.concatenate([mixed_of(i) for i in range(4)], axis=0)
    own_sums = sums_of(mixed_in)
    load_wu.wait()
    pl.semaphore_wait(barrier, len(friends))

    stat = exchange_start(sx_s, own_sums, sx_r, at_x)
    w_start(0, 0)
    for d in (1, 3, 2):
        wu_send(d, 0)
    w_start(0, 1)
    wu_send(1, 1)
    wu_send(3, 1)
    part = exchange_end(stat, sx_s, sx_r)
    stat = exchange_start(sz_s, part, sz_r, at_z)
    w_start(1, 0)
    mean, scale = columns_of(exchange_end(stat, sz_s, sz_r))
    normed = (
        (jnp.concatenate([mixed_of(i) for i in range(4)], axis=0) - mean) * scale * gi[...]
        + bi[...]
    ).astype(BF)
    for i in range(4):
        nloc[i] = normed[i * Q : (i + 1) * Q]

    ncol = (lax.div(z, 2) * 4 + x) * 512 + lax.rem(z, 2) * 256
    mine = nb.at[rows(y * Q, Q, 32), rows(ncol, W, W)]
    nsend = channel()
    for d in (1, 3, 2):
        send(nloc.at[turn(z, d)], mine, at_z(d), nsend)
    nb[rows(y * Q, Q, 32), rows(ncol, W, W)] = nloc[z]
    w_start(3, 0)
    w_forward(0, 0)
    expect(nsend, nloc.at[pl.ds(0, 3)])

    def nblk(h, xx, yy, part):
        col, size = h * 2048 + xx * 512, 512
        if part is not None:
            col, size = col + part * 256, 256
        return nb.at[rows(yy * Q, Q, 32), rows(col, size, 256)]

    a1 = Ring(x, at_x, lambda i, part: nblk(0, i, y, part))
    b1 = Ring(y, at_y, lambda i, part: nblk(1, x, i, part))

    def second(j):
        return (
            Ring(y, at_y, lambda i, part: nblk(0, turn(x, -j), i, part)),
            Ring(x, at_x, lambda i, part: nblk(1, i, turn(y, -j), part)),
        )

    seconds = [second(j) for j in range(4)]

    def n_start(j):
        for ring in seconds[j]:
            ring.start()

    def n_forward(j):
        for ring in seconds[j]:
            ring.forward()

    a1.start()
    b1.start()
    n_start(0)
    w_start(2, 0)
    w_forward(1, 0)
    b1.forward()
    a1.forward()
    n_start(1)
    n_start(3)
    wu_send(2, 1)
    w_start(1, 1)
    w_forward(3, 0)
    w_forward(0, 1)
    n_forward(0)
    b1.finish()
    a1.finish()
    n_start(2)
    w_start(3, 1)
    w_forward(2, 0)
    for u in (0, 1, 3):
        w_finish(u, 0)
    n_forward(1)
    w_forward(1, 1)
    w_start(2, 1)
    w_finish(2, 0)
    w_finish(0, 1)
    n_forward(3)
    w_forward(3, 1)
    n_forward(2)

    wd_a2a, wshare = channel(), channel()
    for d in (1, 3, 2):
        to = turn(x, d)
        part = wd_in.at[rows(to * FS + c * 512, 512, 512), :]
        send(part, wd.at[x, wd_half, :], at_x(d), wd_a2a)
    load_wd.wait()
    w_forward(2, 1)
    for pair in seconds:
        for ring in pair:
            ring.finish()
    shared(0)

    hrings = []

    def up(n):
        cols = slice(n * 256, (n + 1) * 256)
        pre = jnp.dot(nb[...], wu[:, cols], preferred_element_type=F32)
        hid[z, :, cols] = jnp.square(jnp.maximum(pre, 0.0)).astype(BF)

        def hblk(i, half):
            if half is None:
                return hid.at[i, :, pl.ds(n * 256, 256)]
            return hid.at[i, pl.ds(half * 192, 192), pl.ds(n * 256, 256)]

        ring = Ring(z, at_z, hblk)
        ring.start()
        hrings.append(ring)

    up(0)
    for u in (1, 3, 2):
        w_finish(u, 1)
    up(1)
    expect(wd_a2a, wd.at[pl.ds(0, 3), wd_half, :])
    send(wd.at[:, wd_half, :], wd.at[:, wd_half, :], partner, wshare)
    shared(1)
    up(2)
    up(3)
    expect(wshare, wd.at[:, wd_half, :])

    def down(k, group):
        for j in range(4):
            part = jnp.dot(hid[group], wd[j], preferred_element_type=F32)
            for i in range(4):
                pf[k, j, i] = part[i * Q : (i + 1) * Q]
                pb[k, j, i] = part[i * Q : (i + 1) * Q].astype(BF)

    class Reduce:
        def __init__(self, k, kind):
            self.at = (k, kind)
            self.k = k
            self.kind = kind
            self.pos, self.dev = ((y, at_y), (x, at_x))[kind]
            self.pos2, self.dev2 = ((x, at_x), (y, at_y))[kind]

        def item(self, to, first, count):
            if self.kind == 0:
                return (self.k, pl.ds(first, count), to, pl.ds(0, 48), slice(None))
            return (self.k, to, pl.ds(first, count), pl.ds(48, 48), slice(None))

        def first(self):
            far, p, m = turn(self.pos, 2), turn(self.pos, 1), turn(self.pos, -1)
            self.p, self.m = p, m
            self.op = send(pb.at[self.item(far, 0, 2)], opp_p.at[self.at], self.dev(1))
            self.om = send(pb.at[self.item(far, 2, 2)], opp_m.at[self.at], self.dev(-1))
            low, high = pl.ds(0, 2), pl.ds(2, 2)
            self.on_m, self.on_p, self.on_2 = channel(), channel(), channel()
            send(
                pb.at[self.item(p, 2, 2)], from_m.at[(*self.at, high)], self.dev(1), self.on_m
            )
            send(
                pb.at[self.item(m, 0, 2)], from_p.at[(*self.at, low)], self.dev(-1), self.on_p
            )

        def second(self):
            low, high = pl.ds(0, 2), pl.ds(2, 2)
            self.op.wait_recv()
            sum_p[self.at] = (pf[self.item(self.p, 0, 2)] + opp_p[self.at].astype(F32)).astype(BF)
            send(sum_p.at[self.at], from_m.at[(*self.at, low)], self.dev(1), self.on_m)
            self.om.wait_recv()
            sum_m[self.at] = (pf[self.item(self.m, 2, 2)] + opp_m[self.at].astype(F32)).astype(BF)
            send(sum_m.at[self.at], from_p.at[(*self.at, high)], self.dev(-1), self.on_p)

        def third(self):
            expect(self.on_m, from_m.at[self.at])
            expect(self.on_p, from_p.at[self.at])
            total = (
                pf[self.item(self.pos, 0, 4)]
                + from_m[self.at].astype(F32)
                + from_p[self.at].astype(F32)
            )
            rsum[self.at] = total
            tosend[self.at] = total.astype(BF)
            for d in (1, 3, 2):
                to = turn(self.pos2, d)
                send(tosend.at[(*self.at, to)], torecv.at[(*self.at, d - 1)], self.dev2(d), self.on_2)

        def fourth(self, group):
            expect(self.on_2, torecv.at[self.at])
            branch = rsum[(*self.at, self.pos2)]
            for d in range(3):
                branch = branch + torecv[(*self.at, d)].astype(F32)
            part = slice(self.kind * 48, self.kind * 48 + 48)
            mixed = residual_scale * nloc[group, part].astype(F32) + branch
            mo[group, part] = mixed
            mob[y, self.k, part] = mixed.astype(BF)

    groups = [z, turn(z, -1), turn(z, 1), turn(z, 2)]
    reduces = [(Reduce(k, 0), Reduce(k, 1)) for k in range(4)]

    def first(k):
        down(k, groups[k])
        for one in reduces[k]:
            one.first()

    def second_(k):
        for one in reduces[k]:
            one.second()

    def third(k):
        for one in reduces[k]:
            one.third()

    def fourth(k):
        for one in reduces[k]:
            one.fourth(groups[k])

    first(0)
    hrings[0].forward()
    hrings[1].forward()
    second_(0)
    hrings[2].forward()
    third(0)
    hrings[3].forward()
    first(1)
    first(2)
    fourth(0)
    second_(1)
    second_(2)
    third(1)
    third(2)
    for ring in hrings:
        ring.finish()
    first(3)
    second_(3)
    fourth(1)
    fourth(2)
    third(3)

    def mblk(i, half):
        if half is None:
            return mob.at[i, pl.ds(0, 3)]
        return mob.at[i, pl.ds(0, 3), pl.ds(half * 48, 48)]

    ring = Ring(y, at_y, mblk)
    ring.start()
    fourth(3)
    pad = jnp.zeros((32, W), F32)
    mixed_out = jnp.concatenate([a for i in range(4) for a in (mo[i], pad)], axis=0)
    stat = exchange_start(tx_s, sums_of(mixed_out), tx_r, at_x)
    last = channel()
    for d in (1, 3, 2):
        send(mob.at[y, 3], mob.at[y, 3], at_y(d), last)
    part = exchange_end(stat, tx_s, tx_r)
    stat = exchange_start(tz_s, part, tz_r, at_z)
    ring.forward()
    ring.finish()
    expect(last, mob.at[pl.ds(0, 3), 3])
    totals[y] = exchange_end(stat, tz_s, tz_r)
    stat = channel()
    for d in (1, 3, 2):
        send(totals.at[y], totals.at[y], at_y(d), stat)

    def finish(yy):
        for k in range(4):
            mean, scale = columns_of(totals[yy, :, rows(groups[k] * 128, 128, 128)])
            block = (mob[yy, k].astype(F32) - mean[0:Q]) * scale[0:Q] * go[...] + bo[...]
            obuf[yy, k] = block.astype(BF)
            fetch(obuf.at[yy, k], out.at[groups[k], yy], 4)

    finish(y)
    expect(stat, totals.at[pl.ds(0, 3)])
    for d in (1, 3, 2):
        finish(turn(y, -d))
    assert len(used) == N_RECV, len(used)
    for copy in remote[-N_SEND:]:
        copy.wait_send()
    pltpu.make_async_copy(obuf, out, local_sem.at[4]).wait()


N_SEND = 64
N_RECV = 126
N_LOCAL = 5


def per_device(carried, branch_in, gain_in, bias_in, up_weight, down_weight, gain_out, bias_out):
    any_spec = pl.BlockSpec(memory_space=pl.ANY)
    vmem_spec = pl.BlockSpec(memory_space=pltpu.VMEM)
    V = pltpu.VMEM
    result = pl.pallas_call(
        kernel,
        out_shape=jax.ShapeDtypeStruct((4, 4, Q, W), BF),
        in_specs=[any_spec, any_spec, vmem_spec, vmem_spec, any_spec, any_spec, vmem_spec, vmem_spec],
        out_specs=any_spec,
        scratch_shapes=[
            V((4, Q, W), BF), V((4, Q, W), BF), V((4, Q, W), BF),
            V((G, D), BF), V((D, FS), BF), V((4, FS, W), BF), V((4, G, FS), BF),
            V((4, 4, 4, Q, W), F32), V((4, 4, 4, Q, W), BF),
            *[V((4, 2, 2, 48, W), BF) for _ in range(4)],
            V((4, 2, 4, 48, W), BF), V((4, 2, 4, 48, W), BF),
            V((4, 2, 4, 48, W), F32), V((4, 2, 4, 48, W), BF), V((4, 2, 3, 48, W), BF),
            V((4, Q, W), F32), V((4, 4, Q, W), BF), V((4, 4, Q, W), BF),
            *[V(shape, F32) for shape in ((8, G), (3, 8, G)) * 2],
            *[V(shape, F32) for shape in ((8, 512), (3, 8, 512)) * 2],
            V((4, 8, 512), F32),
            pltpu.SemaphoreType.DMA((N_SEND,)),
            pltpu.SemaphoreType.DMA((N_RECV,)),
            pltpu.SemaphoreType.DMA((N_LOCAL,)),
        ],
        compiler_params=pltpu.CompilerParams(
            collective_id=0, has_side_effects=True, vmem_limit_bytes=60 * 1024 * 1024
        ),
    )(
        carried.reshape(4, 4, Q, W), branch_in.reshape(4, 4, Q, W),
        gain_in.reshape(1, W), bias_in.reshape(1, W), up_weight, down_weight,
        gain_out.reshape(1, W), bias_out.reshape(1, W),
    )
    return result.reshape(carried.shape)


def solution(mesh):
    in_specs = (
        P("dp", "ra"),
        P("dp", "ra"),
        P("ra"),
        P("ra"),
        P("ra", "cb"),
        P("cb", "ra"),
        P("ra"),
        P("ra"),
    )
    out_specs = P("dp", "ra")
    return jax.shard_map(
        per_device, mesh=mesh, in_specs=in_specs, out_specs=out_specs, check_vma=False
    )
```

```python
import functools

import jax
import jax.numpy as jnp
from jax import lax
from jax.experimental import pallas as pl
from jax.experimental.pallas import tpu as pltpu
from jax.sharding import PartitionSpec as P

residual_scale = 2.0**0.25
norm_eps = 1e-05
MESH = pl.DeviceIdType.MESH
BF = jnp.bfloat16
F32 = jnp.float32

Q = 96
G = 4 * Q
W = 256
D = 16 * W
FS = 1024


def kernel(
    car, bra, gi, bi, wu_in, wd_in, go, bo, out,
    cbuf, bbuf, nloc, nb, wu, wd, hid, pf, pb, opp_p, opp_m, sum_p, sum_m,
    from_m, from_p, rsum, tosend, torecv, mo, mob, obuf,
    sx_s, sx_r, tx_s, tx_r, totals, picked,
    send_sem, recv_sem, local_sem, hello,
):
    r = lax.axis_index("ra")
    y = lax.axis_index("cb")
    c = lax.axis_index("dp")
    z = lax.div(r, 4)
    x = lax.rem(r, 4)

    def turn(i, d):
        return lax.rem(i + d + 4, 4)

    def at_x(d):
        return (z * 4 + turn(x, d), y, c)

    def at_z(d):
        return (turn(z, d) * 4 + x, y, c)

    def at_y(d):
        return (r, turn(y, d), c)

    def at_zx(d):
        return (turn(z, d // 4) * 4 + turn(x, d % 4), y, c)

    def at_zy(d):
        return (turn(z, d // 4) * 4 + x, turn(y, d % 4), c)

    partner = (r, y, 1 - c)
    remote = []
    local = []

    used = []

    def channel():
        used.append(len(used))
        return used[-1]

    def described(src, dst, device, slot, on):
        return pltpu.make_async_remote_copy(
            src_ref=src, dst_ref=dst, send_sem=send_sem.at[slot], recv_sem=recv_sem.at[on],
            device_id=device, device_id_type=MESH,
        )

    def send(src, dst, device, on=None):
        k = len(remote)
        if k >= N_SEND:
            remote[k - N_SEND].wait_send()
        copy = described(src, dst, device, k % N_SEND, channel() if on is None else on)
        copy.start()
        remote.append(copy)
        return copy

    def expect(on, cover):
        described(cover, cover, partner, 0, on).wait_recv()

    def fetch(src, dst, on=None):
        k = len(local) if on is None else on
        copy = pltpu.make_async_copy(src, dst, local_sem.at[k])
        copy.start()
        local.append(copy)
        return copy

    class Ring:
        def __init__(self, pos, dev, blk):
            self.pos, self.dev, self.blk = pos, dev, blk

        def start(self):
            mine = self.blk(self.pos, None)
            self.p = send(mine, mine, self.dev(1))
            self.m = send(mine, mine, self.dev(-1))

        def forward(self):
            self.on = channel()
            self.p.wait_recv()
            half = self.blk(turn(self.pos, -1), 0)
            send(half, half, self.dev(1), self.on)
            self.m.wait_recv()
            half = self.blk(turn(self.pos, 1), 1)
            send(half, half, self.dev(-1), self.on)

        def finish(self):
            expect(self.on, self.blk(turn(self.pos, 2), None))

    def rows(start, size, step):
        return pl.ds(pl.multiple_of(start, step), size)

    load_c = fetch(car.at[:, y], cbuf)
    load_b = fetch(bra.at[:, y], bbuf)

    def wrow(zz, xx, cc):
        return (lax.div(zz, 2) * 4 + xx) * 512 + lax.rem(zz, 2) * 256 + cc * 128

    def wblk(zz, xx, f, half=None):
        start = wrow(zz, xx, c)
        if half is None:
            return wu.at[rows(start, 128, 128), pl.ds(f * 512, 512)]
        return wu.at[rows(start + half * 64, 64, 64), pl.ds(f * 512, 512)]

    load_wu = fetch(
        wu_in.at[rows(c * 128, 128, 128), rows(x * FS, FS, FS)],
        wu.at[rows(wrow(z, x, c), 128, 128), :],
    )
    wd_half = rows(c * 512, 512, 512)
    load_wd = fetch(wd_in.at[rows(x * FS + c * 512, 512, 512), :], wd.at[x, wd_half, :])

    barrier = pltpu.get_barrier_semaphore()
    friends = [at_zx(d) for d in range(1, 16)] + [at_zy(d) for d in range(1, 16) if d % 4]
    for device in friends:
        pl.semaphore_signal(barrier, inc=1, device_id=device, device_id_type=MESH)

    @pl.when(c == 0)
    def _():
        pl.semaphore_signal(barrier, inc=1, device_id=partner, device_id_type=MESH)

    def mixed_of(i):
        return residual_scale * cbuf[i].astype(F32) + bbuf[i].astype(F32)

    def sums_of(mixed):
        total = jnp.sum(mixed, axis=1, keepdims=True)
        square = jnp.sum(mixed * mixed, axis=1, keepdims=True)
        lane = lax.broadcasted_iota(jnp.int32, (mixed.shape[0], 128), 1)
        return jnp.transpose(jnp.where(lane == 0, total, square))[0:8]

    def columns_of(sums):
        row = lax.broadcasted_iota(jnp.int32, (128, sums.shape[1]), 0)
        spread = jnp.transpose(jnp.where(row == 0, sums[0:1], sums[1:2]))
        mean = spread[:, 0:1] / D
        var = spread[:, 1:2] / D - mean * mean
        return mean, lax.rsqrt(var + norm_eps)

    def exchange_start(buf, own, got, dev, n):
        buf[...] = own
        on = channel()
        for d in range(1, n):
            send(buf, got.at[d - 1], dev(d), on)
        return on

    def exchange_end(on, buf, got):
        expect(on, got)
        return sum((got[d] for d in range(got.shape[0])), buf[...])

    d2d = (channel(), channel())

    held = []

    def share(zz, xx, f):
        if held is None:
            send(wblk(zz, xx, f), wblk(zz, xx, f), partner, d2d[f])
        else:
            held.append((zz, xx, f))

    def share_held():
        nonlocal held

        @pl.when(c == 0)
        def _():
            pl.semaphore_wait(hello, 1)

        ready, held = held, None
        for one in ready:
            share(*one)

    def shared(f):
        expect(d2d[f], wu.at[pl.ds(0, D // 2), pl.ds(f * 512, 512)])

    def wring(u, f):
        xx = turn(x, -u)
        return Ring(z, at_z, lambda i, half: wblk(i, xx, f, half))

    wrings = {(u, f): wring(u, f) for u in range(4) for f in range(2)}
    a2a = {}

    def wu_send(d, f):
        cols = rows(turn(x, d) * FS + f * 512, 512, 512)
        a2a[d, f] = send(wu_in.at[rows(c * 128, 128, 128), cols], wblk(z, x, f), at_x(d))

    def w_start(u, f):
        if u:
            a2a[u, f].wait_recv()
        wrings[u, f].start()
        share(z, turn(x, -u), f)

    def w_forward(u, f):
        wrings[u, f].forward()
        share(turn(z, -1), turn(x, -u), f)
        share(turn(z, 1), turn(x, -u), f)

    def w_finish(u, f):
        wrings[u, f].finish()
        share(turn(z, 2), turn(x, -u), f)

    load_c.wait()
    load_b.wait()
    mixed_in = jnp.concatenate([mixed_of(i) for i in range(4)], axis=0)
    own_sums = sums_of(mixed_in)
    load_wu.wait()
    pl.semaphore_wait(barrier, len(friends) + c)

    @pl.when(c == 1)
    def _():
        pl.semaphore_signal(hello, inc=1, device_id=partner, device_id_type=MESH)

    stat = exchange_start(sx_s, own_sums, sx_r, at_zx, 16)
    w_start(0, 0)
    for d in (1, 3, 2):
        wu_send(d, 0)
    w_start(0, 1)
    wu_send(1, 1)
    wu_send(3, 1)
    mean, scale = columns_of(exchange_end(stat, sx_s, sx_r))
    normed = (
        (jnp.concatenate([mixed_of(i) for i in range(4)], axis=0) - mean) * scale * gi[...]
        + bi[...]
    ).astype(BF)
    for i in range(4):
        nloc[i] = normed[i * Q : (i + 1) * Q]

    ncol = (lax.div(z, 2) * 4 + x) * 512 + lax.rem(z, 2) * 256
    mine = nb.at[rows(y * Q, Q, 32), rows(ncol, W, W)]
    nsend = channel()
    for d in (1, 3, 2):
        send(nloc.at[turn(z, d)], mine, at_z(d), nsend)
    nb[rows(y * Q, Q, 32), rows(ncol, W, W)] = nloc[z]
    w_start(1, 0)
    w_start(3, 0)
    w_forward(0, 0)
    expect(nsend, nloc.at[pl.ds(0, 3)])

    def nblk(h, xx, yy, part):
        col, size = h * 2048 + xx * 512, 512
        if part is not None:
            col, size = col + part * 256, 256
        return nb.at[rows(yy * Q, Q, 32), rows(col, size, 256)]

    a1 = Ring(x, at_x, lambda i, part: nblk(0, i, y, part))
    b1 = Ring(y, at_y, lambda i, part: nblk(1, x, i, part))

    def second(j):
        return (
            Ring(y, at_y, lambda i, part: nblk(0, turn(x, -j), i, part)),
            Ring(x, at_x, lambda i, part: nblk(1, i, turn(y, -j), part)),
        )

    seconds = [second(j) for j in range(4)]

    def n_start(j):
        for ring in seconds[j]:
            ring.start()

    def n_forward(j):
        for ring in seconds[j]:
            ring.forward()

    a1.start()
    b1.start()
    n_start(0)
    w_start(2, 0)
    w_forward(1, 0)
    b1.forward()
    a1.forward()
    n_start(1)
    n_start(3)
    share_held()
    wu_send(2, 1)
    w_start(1, 1)
    w_forward(3, 0)
    w_forward(0, 1)
    n_forward(0)
    b1.finish()
    a1.finish()
    n_start(2)
    w_start(3, 1)
    w_forward(2, 0)
    for u in (0, 1, 3):
        w_finish(u, 0)
    n_forward(1)
    w_forward(1, 1)
    w_start(2, 1)
    w_finish(2, 0)
    w_finish(0, 1)
    n_forward(3)
    w_forward(3, 1)
    n_forward(2)

    wd_a2a, wshare = channel(), channel()
    for d in (1, 3, 2):
        to = turn(x, d)
        part = wd_in.at[rows(to * FS + c * 512, 512, 512), :]
        send(part, wd.at[x, wd_half, :], at_x(d), wd_a2a)
    load_wd.wait()
    w_forward(2, 1)
    for pair in seconds:
        for ring in pair:
            ring.finish()
    shared(0)

    hrings = []

    def up(n):
        cols = slice(n * 256, (n + 1) * 256)
        pre = sum(
            jnp.dot(nb[:, i : i + 1024], wu[i : i + 1024, cols], preferred_element_type=F32)
            for i in range(0, D, 1024)
        )
        hid[z, :, cols] = jnp.square(jnp.maximum(pre, 0.0)).astype(BF)

        def hblk(i, half):
            if half is None:
                return hid.at[i, :, pl.ds(n * 256, 256)]
            return hid.at[i, pl.ds(half * 192, 192), pl.ds(n * 256, 256)]

        ring = Ring(z, at_z, hblk)
        ring.start()
        hrings.append(ring)

    up(0)
    for u in (1, 3, 2):
        w_finish(u, 1)
    up(1)
    expect(wd_a2a, wd.at[pl.ds(0, 3), wd_half, :])
    send(wd.at[:, wd_half, :], wd.at[:, wd_half, :], partner, wshare)
    shared(1)
    up(2)
    up(3)
    expect(wshare, wd.at[:, wd_half, :])

    def down(k, group):
        for j in range(4):
            part = jnp.dot(hid[group], wd[j], preferred_element_type=F32)
            for i in range(4):
                pf[k, j, i] = part[i * Q : (i + 1) * Q]
                pb[k, j, i] = part[i * Q : (i + 1) * Q].astype(BF)

    class Reduce:
        def __init__(self, k, kind):
            self.at = (k, kind)
            self.k = k
            self.kind = kind
            self.pos, self.dev = ((y, at_y), (x, at_x))[kind]
            self.pos2, self.dev2 = ((x, at_x), (y, at_y))[kind]

        def item(self, to, first, count):
            if self.kind == 0:
                return (self.k, pl.ds(first, count), to, pl.ds(0, 48), slice(None))
            return (self.k, to, pl.ds(first, count), pl.ds(48, 48), slice(None))

        def first(self):
            far, p, m = turn(self.pos, 2), turn(self.pos, 1), turn(self.pos, -1)
            self.p, self.m = p, m
            self.op = send(pb.at[self.item(far, 0, 2)], opp_p.at[self.at], self.dev(1))
            self.om = send(pb.at[self.item(far, 2, 2)], opp_m.at[self.at], self.dev(-1))
            low, high = pl.ds(0, 2), pl.ds(2, 2)
            self.on_m, self.on_p, self.on_2 = channel(), channel(), channel()
            send(
                pb.at[self.item(p, 2, 2)], from_m.at[(*self.at, high)], self.dev(1), self.on_m
            )
            send(
                pb.at[self.item(m, 0, 2)], from_p.at[(*self.at, low)], self.dev(-1), self.on_p
            )

        def second(self):
            low, high = pl.ds(0, 2), pl.ds(2, 2)
            self.op.wait_recv()
            sum_p[self.at] = (pf[self.item(self.p, 0, 2)] + opp_p[self.at].astype(F32)).astype(BF)
            send(sum_p.at[self.at], from_m.at[(*self.at, low)], self.dev(1), self.on_m)
            self.om.wait_recv()
            sum_m[self.at] = (pf[self.item(self.m, 2, 2)] + opp_m[self.at].astype(F32)).astype(BF)
            send(sum_m.at[self.at], from_p.at[(*self.at, high)], self.dev(-1), self.on_p)

        def third(self):
            expect(self.on_m, from_m.at[self.at])
            expect(self.on_p, from_p.at[self.at])
            total = (
                pf[self.item(self.pos, 0, 4)]
                + from_m[self.at].astype(F32)
                + from_p[self.at].astype(F32)
            )
            rsum[self.at] = total
            tosend[self.at] = total.astype(BF)
            for d in (1, 3, 2):
                to = turn(self.pos2, d)
                send(tosend.at[(*self.at, to)], torecv.at[(*self.at, d - 1)], self.dev2(d), self.on_2)

        def fourth(self, group):
            expect(self.on_2, torecv.at[self.at])
            branch = rsum[(*self.at, self.pos2)]
            for d in range(3):
                branch = branch + torecv[(*self.at, d)].astype(F32)
            part = slice(self.kind * 48, self.kind * 48 + 48)
            mixed = residual_scale * nloc[group, part].astype(F32) + branch
            mo[group, part] = mixed
            mob[y, self.k, part] = mixed.astype(BF)

    groups = [z, turn(z, -1), turn(z, 1), turn(z, 2)]
    reduces = [(Reduce(k, 0), Reduce(k, 1)) for k in range(4)]

    def first(k):
        down(k, groups[k])
        for one in reduces[k]:
            one.first()

    def second_(k):
        for one in reduces[k]:
            one.second()

    def third(k):
        for one in reduces[k]:
            one.third()

    def fourth(k):
        for one in reduces[k]:
            one.fourth(groups[k])

    first(0)
    hrings[0].forward()
    hrings[1].forward()
    second_(0)
    hrings[2].forward()
    third(0)
    hrings[3].forward()
    first(1)
    first(2)
    fourth(0)
    second_(1)
    second_(2)
    third(1)
    third(2)
    for ring in hrings:
        ring.finish()
    first(3)
    second_(3)
    fourth(1)
    fourth(2)
    third(3)

    def mblk(i, half):
        if half is None:
            return mob.at[i, pl.ds(0, 3)]
        return mob.at[i, pl.ds(0, 3), pl.ds(half * 48, 48)]

    ring = Ring(y, at_y, mblk)
    ring.start()
    fourth(3)
    pad = jnp.zeros((32, W), F32)
    mixed_out = jnp.concatenate([a for i in range(4) for a in (mo[i], pad)], axis=0)
    stat = exchange_start(tx_s, sums_of(mixed_out), tx_r, at_x, 4)
    last = channel()
    for d in (1, 3, 2):
        send(mob.at[y, 3], mob.at[y, 3], at_y(d), last)
    ring.forward()
    totals[0] = exchange_end(stat, tx_s, tx_r)
    stat = channel()
    for d in range(1, 16):
        send(totals.at[0], totals.at[d], at_zy(d), stat)
    ring.finish()
    expect(last, mob.at[pl.ds(0, 3), 3])
    expect(stat, totals.at[pl.ds(1, 15)])
    stacked = []
    for dy in range(4):
        sums = totals[dy] + totals[4 + dy] + totals[8 + dy] + totals[12 + dy]
        picked[dy] = sums
        for k in range(4):
            stacked.append(picked[dy, :, rows(groups[k] * 128, 128, 128)])
    columns = jnp.transpose(jnp.concatenate(stacked, axis=0))[0:Q]
    for dy in range(4):
        yy = turn(y, -dy)
        for k in range(4):
            at = (dy * 4 + k) * 8
            mean = columns[:, at : at + 1] / D
            var = columns[:, at + 1 : at + 2] / D - mean * mean
            block = (mob[yy, k].astype(F32) - mean) * lax.rsqrt(var + norm_eps)
            obuf[yy, k] = (block * go[...] + bo[...]).astype(BF)
            fetch(obuf.at[yy, k], out.at[groups[k], yy], 4)
    assert len(used) == N_RECV, len(used)
    for copy in remote[-N_SEND:]:
        copy.wait_send()
    pltpu.make_async_copy(obuf, out, local_sem.at[4]).wait()


N_SEND = 64
N_RECV = 124
N_LOCAL = 5


def per_device(carried, branch_in, gain_in, bias_in, up_weight, down_weight, gain_out, bias_out):
    any_spec = pl.BlockSpec(memory_space=pl.ANY)
    vmem_spec = pl.BlockSpec(memory_space=pltpu.VMEM)
    V = pltpu.VMEM
    result = pl.pallas_call(
        kernel,
        out_shape=jax.ShapeDtypeStruct((4, 4, Q, W), BF),
        in_specs=[any_spec, any_spec, vmem_spec, vmem_spec, any_spec, any_spec, vmem_spec, vmem_spec],
        out_specs=any_spec,
        scratch_shapes=[
            V((4, Q, W), BF), V((4, Q, W), BF), V((4, Q, W), BF),
            V((G, D), BF), V((D, FS), BF), V((4, FS, W), BF), V((4, G, FS), BF),
            V((4, 4, 4, Q, W), F32), V((4, 4, 4, Q, W), BF),
            *[V((4, 2, 2, 48, W), BF) for _ in range(4)],
            V((4, 2, 4, 48, W), BF), V((4, 2, 4, 48, W), BF),
            V((4, 2, 4, 48, W), F32), V((4, 2, 4, 48, W), BF), V((4, 2, 3, 48, W), BF),
            V((4, Q, W), F32), V((4, 4, Q, W), BF), V((4, 4, Q, W), BF),
            V((8, G), F32), V((15, 8, G), F32),
            V((8, 512), F32), V((3, 8, 512), F32), V((16, 8, 512), F32), V((4, 8, 512), F32),
            pltpu.SemaphoreType.DMA((N_SEND,)),
            pltpu.SemaphoreType.DMA((N_RECV,)),
            pltpu.SemaphoreType.DMA((N_LOCAL,)),
            pltpu.SemaphoreType.REGULAR,
        ],
        compiler_params=pltpu.CompilerParams(
            collective_id=0, has_side_effects=True, vmem_limit_bytes=60 * 1024 * 1024
        ),
    )(
        carried.reshape(4, 4, Q, W), branch_in.reshape(4, 4, Q, W),
        gain_in.reshape(1, W), bias_in.reshape(1, W), up_weight, down_weight,
        gain_out.reshape(1, W), bias_out.reshape(1, W),
    )
    return result.reshape(carried.shape)


def solution(mesh):
    in_specs = (
        P("dp", "ra"),
        P("dp", "ra"),
        P("ra"),
        P("ra"),
        P("ra", "cb"),
        P("cb", "ra"),
        P("ra"),
        P("ra"),
    )
    out_specs = P("dp", "ra")
    return jax.shard_map(
        per_device, mesh=mesh, in_specs=in_specs, out_specs=out_specs, check_vma=False
    )
```

```python
import functools

import jax
import jax.numpy as jnp
from jax import lax
from jax.experimental import pallas as pl
from jax.experimental.pallas import tpu as pltpu
from jax.sharding import PartitionSpec as P

residual_scale = 2.0**0.25
norm_eps = 1e-05
MESH = pl.DeviceIdType.MESH
BF = jnp.bfloat16
F32 = jnp.float32

Q = 96
G = 4 * Q
W = 256
D = 16 * W
FS = 1024


def kernel(
    car, bra, gi, bi, wu_in, wd_in, go, bo, out,
    cbuf, bbuf, nloc, nb, wu, wd, hid, pf, pb, opp_p, opp_m, sum_p, sum_m,
    from_m, from_p, rsum, tosend, torecv, mo, mob, obuf,
    sx_s, sx_r, tx_s, tx_r, totals,
    send_sem, recv_sem, local_sem, hello,
):
    r = lax.axis_index("ra")
    y = lax.axis_index("cb")
    c = lax.axis_index("dp")
    z = lax.div(r, 4)
    x = lax.rem(r, 4)

    def turn(i, d):
        return lax.rem(i + d + 4, 4)

    def at_x(d):
        return (z * 4 + turn(x, d), y, c)

    def at_z(d):
        return (turn(z, d) * 4 + x, y, c)

    def at_y(d):
        return (r, turn(y, d), c)

    def at_zx(d):
        return (turn(z, d // 4) * 4 + turn(x, d % 4), y, c)

    def at_zy(d):
        return (turn(z, d // 4) * 4 + x, turn(y, d % 4), c)

    partner = (r, y, 1 - c)
    remote = []
    local = []

    used = []

    def channel():
        used.append(len(used))
        return used[-1]

    def described(src, dst, device, slot, on):
        return pltpu.make_async_remote_copy(
            src_ref=src, dst_ref=dst, send_sem=send_sem.at[slot], recv_sem=recv_sem.at[on],
            device_id=device, device_id_type=MESH,
        )

    def send(src, dst, device, on=None):
        k = len(remote)
        if k >= N_SEND:
            remote[k - N_SEND].wait_send()
        copy = described(src, dst, device, k % N_SEND, channel() if on is None else on)
        copy.start()
        remote.append(copy)
        return copy

    def expect(on, cover):
        described(cover, cover, partner, 0, on).wait_recv()

    def fetch(src, dst, on=None):
        k = len(local) if on is None else on
        copy = pltpu.make_async_copy(src, dst, local_sem.at[k])
        copy.start()
        local.append(copy)
        return copy

    class Ring:
        def __init__(self, pos, dev, blk):
            self.pos, self.dev, self.blk = pos, dev, blk

        def start(self):
            mine = self.blk(self.pos, None)
            self.p = send(mine, mine, self.dev(1))
            self.m = send(mine, mine, self.dev(-1))

        def forward(self):
            self.on = channel()
            self.p.wait_recv()
            half = self.blk(turn(self.pos, -1), 0)
            send(half, half, self.dev(1), self.on)
            self.m.wait_recv()
            half = self.blk(turn(self.pos, 1), 1)
            send(half, half, self.dev(-1), self.on)

        def finish(self):
            expect(self.on, self.blk(turn(self.pos, 2), None))

    def rows(start, size, step):
        return pl.ds(pl.multiple_of(start, step), size)

    load_c = fetch(car.at[:, y], cbuf)
    load_b = fetch(bra.at[:, y], bbuf)

    def wrow(zz, xx, cc):
        return (lax.div(zz, 2) * 4 + xx) * 512 + lax.rem(zz, 2) * 256 + cc * 128

    def wblk(zz, xx, f, half=None):
        start = wrow(zz, xx, c)
        if half is None:
            return wu.at[rows(start, 128, 128), pl.ds(f * 512, 512)]
        return wu.at[rows(start + half * 64, 64, 64), pl.ds(f * 512, 512)]

    load_wu = fetch(
        wu_in.at[rows(c * 128, 128, 128), rows(x * FS, FS, FS)],
        wu.at[rows(wrow(z, x, c), 128, 128), :],
    )
    wd_half = rows(c * 512, 512, 512)
    load_wd = fetch(wd_in.at[rows(x * FS + c * 512, 512, 512), :], wd.at[x, wd_half, :])

    barrier = pltpu.get_barrier_semaphore()
    friends = [at_zx(d) for d in range(1, 16)] + [at_zy(d) for d in range(1, 16) if d % 4]
    for device in friends:
        pl.semaphore_signal(barrier, inc=1, device_id=device, device_id_type=MESH)

    @pl.when(c == 0)
    def _():
        pl.semaphore_signal(barrier, inc=1, device_id=partner, device_id_type=MESH)

    def mixed_of(i):
        return residual_scale * cbuf[i].astype(F32) + bbuf[i].astype(F32)

    def sums_of(groups):
        lane = lax.broadcasted_iota(jnp.int32, (128, 128), 1)
        packed = jnp.zeros((128, 128), F32)
        pad = jnp.zeros((32, 1), F32)
        for g, mixed in enumerate(groups):
            total = jnp.sum(mixed, axis=1, keepdims=True)
            square = jnp.sum(mixed * mixed, axis=1, keepdims=True)
            packed = jnp.where(lane == g, jnp.concatenate([total, pad], axis=0), packed)
            packed = jnp.where(lane == 4 + g, jnp.concatenate([square, pad], axis=0), packed)
        return jnp.transpose(packed)[0:8]

    def columns_of(sums):
        return jnp.transpose(jnp.concatenate(sums + [sums[0]] * (16 - len(sums)), axis=0))[0:Q]

    def moments(columns, at):
        mean = columns[:, at : at + 1] / D
        var = columns[:, at + 4 : at + 5] / D - mean * mean
        return mean, lax.rsqrt(var + norm_eps)

    def exchange_start(buf, own, got, dev, n):
        buf[...] = own
        on = channel()
        for d in range(1, n):
            send(buf, got.at[d - 1], dev(d), on)
        return on

    def exchange_end(on, buf, got):
        expect(on, got)
        return sum((got[d] for d in range(got.shape[0])), buf[...])

    d2d = (channel(), channel())

    held = []

    def share(zz, xx, f):
        if held is None:
            send(wblk(zz, xx, f), wblk(zz, xx, f), partner, d2d[f])
        else:
            held.append((zz, xx, f))

    def share_held():
        nonlocal held

        @pl.when(c == 0)
        def _():
            pl.semaphore_wait(hello, 1)

        ready, held = held, None
        for one in ready:
            share(*one)

    def shared(f):
        expect(d2d[f], wu.at[pl.ds(0, D // 2), pl.ds(f * 512, 512)])

    def wring(u, f):
        xx = turn(x, -u)
        return Ring(z, at_z, lambda i, half: wblk(i, xx, f, half))

    wrings = {(u, f): wring(u, f) for u in range(4) for f in range(2)}
    a2a = {}

    def wu_send(d, f):
        cols = rows(turn(x, d) * FS + f * 512, 512, 512)
        a2a[d, f] = send(wu_in.at[rows(c * 128, 128, 128), cols], wblk(z, x, f), at_x(d))

    def w_start(u, f):
        if u:
            a2a[u, f].wait_recv()
        wrings[u, f].start()
        share(z, turn(x, -u), f)

    def w_forward(u, f):
        wrings[u, f].forward()
        share(turn(z, -1), turn(x, -u), f)
        share(turn(z, 1), turn(x, -u), f)

    def w_finish(u, f):
        wrings[u, f].finish()
        share(turn(z, 2), turn(x, -u), f)

    load_c.wait()
    load_b.wait()
    own_sums = sums_of([mixed_of(i) for i in range(4)])
    load_wu.wait()
    pl.semaphore_wait(barrier, len(friends) + c)

    @pl.when(c == 1)
    def _():
        pl.semaphore_signal(hello, inc=1, device_id=partner, device_id_type=MESH)

    stat = exchange_start(sx_s, own_sums, sx_r, at_zx, 16)
    w_start(0, 0)
    for d in (1, 3, 2):
        wu_send(d, 0)
    w_start(0, 1)
    wu_send(1, 1)
    wu_send(3, 1)
    columns = columns_of([exchange_end(stat, sx_s, sx_r)])
    for i in range(4):
        mean, scale = moments(columns, i)
        nloc[i] = ((mixed_of(i) - mean) * scale * gi[...] + bi[...]).astype(BF)

    ncol = (lax.div(z, 2) * 4 + x) * 512 + lax.rem(z, 2) * 256
    mine = nb.at[rows(y * Q, Q, 32), rows(ncol, W, W)]
    nsend = channel()
    for d in (1, 3, 2):
        send(nloc.at[turn(z, d)], mine, at_z(d), nsend)
    nb[rows(y * Q, Q, 32), rows(ncol, W, W)] = nloc[z]
    w_start(1, 0)
    w_start(3, 0)
    w_forward(0, 0)
    expect(nsend, nloc.at[pl.ds(0, 3)])

    def nblk(h, xx, yy, part):
        col, size = h * 2048 + xx * 512, 512
        if part is not None:
            col, size = col + part * 256, 256
        return nb.at[rows(yy * Q, Q, 32), rows(col, size, 256)]

    a1 = Ring(x, at_x, lambda i, part: nblk(0, i, y, part))
    b1 = Ring(y, at_y, lambda i, part: nblk(1, x, i, part))

    def second(j):
        return (
            Ring(y, at_y, lambda i, part: nblk(0, turn(x, -j), i, part)),
            Ring(x, at_x, lambda i, part: nblk(1, i, turn(y, -j), part)),
        )

    seconds = [second(j) for j in range(4)]

    def n_start(j):
        for ring in seconds[j]:
            ring.start()

    def n_forward(j):
        for ring in seconds[j]:
            ring.forward()

    a1.start()
    b1.start()
    n_start(0)
    wu_send(2, 1)
    w_start(2, 0)
    w_forward(0, 1)
    w_start(3, 1)
    w_forward(1, 0)
    b1.forward()
    a1.forward()
    n_start(1)
    n_start(3)
    w_start(1, 1)
    w_forward(3, 0)
    share_held()
    n_forward(0)
    b1.finish()
    a1.finish()
    n_start(2)
    w_start(2, 1)
    w_forward(2, 0)
    n_forward(1)
    n_forward(3)
    w_forward(3, 1)
    n_forward(2)
    w_forward(1, 1)

    wd_a2a, wshare = channel(), channel()
    for d in (1, 3, 2):
        to = turn(x, d)
        part = wd_in.at[rows(to * FS + c * 512, 512, 512), :]
        send(part, wd.at[x, wd_half, :], at_x(d), wd_a2a)
    load_wd.wait()
    for u in range(4):
        w_finish(u, 0)
    for pair in seconds:
        for ring in pair:
            ring.finish()
    w_forward(2, 1)
    shared(0)

    hrings = []

    def up(n):
        cols = slice(n * 256, (n + 1) * 256)
        pre = sum(
            jnp.dot(nb[:, i : i + 1024], wu[i : i + 1024, cols], preferred_element_type=F32)
            for i in range(0, D, 1024)
        )
        hid[z, :, cols] = jnp.square(jnp.maximum(pre, 0.0)).astype(BF)

        def hblk(i, half):
            if half is None:
                return hid.at[i, :, pl.ds(n * 256, 256)]
            return hid.at[i, pl.ds(half * 192, 192), pl.ds(n * 256, 256)]

        ring = Ring(z, at_z, hblk)
        ring.start()
        hrings.append(ring)

    up(0)
    for u in (0, 3, 1, 2):
        w_finish(u, 1)
    up(1)
    expect(wd_a2a, wd.at[pl.ds(0, 3), wd_half, :])
    send(wd.at[:, wd_half, :], wd.at[:, wd_half, :], partner, wshare)
    shared(1)
    up(2)
    up(3)
    expect(wshare, wd.at[:, wd_half, :])

    def down(k, group):
        for j in range(4):
            part = jnp.dot(hid[group], wd[j], preferred_element_type=F32)
            for i in range(4):
                pf[k, j, i] = part[i * Q : (i + 1) * Q]
                pb[k, j, i] = part[i * Q : (i + 1) * Q].astype(BF)

    class Reduce:
        def __init__(self, k, kind):
            self.at = (k, kind)
            self.k = k
            self.kind = kind
            self.pos, self.dev = ((y, at_y), (x, at_x))[kind]
            self.pos2, self.dev2 = ((x, at_x), (y, at_y))[kind]

        def item(self, to, first, count):
            if self.kind == 0:
                return (self.k, pl.ds(first, count), to, pl.ds(0, 48), slice(None))
            return (self.k, to, pl.ds(first, count), pl.ds(48, 48), slice(None))

        def first(self):
            far, p, m = turn(self.pos, 2), turn(self.pos, 1), turn(self.pos, -1)
            self.p, self.m = p, m
            self.op = send(pb.at[self.item(far, 0, 2)], opp_p.at[self.at], self.dev(1))
            self.om = send(pb.at[self.item(far, 2, 2)], opp_m.at[self.at], self.dev(-1))
            low, high = pl.ds(0, 2), pl.ds(2, 2)
            self.on_m, self.on_p, self.on_2 = channel(), channel(), channel()
            send(
                pb.at[self.item(p, 2, 2)], from_m.at[(*self.at, high)], self.dev(1), self.on_m
            )
            send(
                pb.at[self.item(m, 0, 2)], from_p.at[(*self.at, low)], self.dev(-1), self.on_p
            )

        def second(self):
            low, high = pl.ds(0, 2), pl.ds(2, 2)
            self.op.wait_recv()
            sum_p[self.at] = (pf[self.item(self.p, 0, 2)] + opp_p[self.at].astype(F32)).astype(BF)
            send(sum_p.at[self.at], from_m.at[(*self.at, low)], self.dev(1), self.on_m)
            self.om.wait_recv()
            sum_m[self.at] = (pf[self.item(self.m, 2, 2)] + opp_m[self.at].astype(F32)).astype(BF)
            send(sum_m.at[self.at], from_p.at[(*self.at, high)], self.dev(-1), self.on_p)

        def third(self):
            expect(self.on_m, from_m.at[self.at])
            expect(self.on_p, from_p.at[self.at])
            total = (
                pf[self.item(self.pos, 0, 4)]
                + from_m[self.at].astype(F32)
                + from_p[self.at].astype(F32)
            )
            rsum[self.at] = total
            tosend[self.at] = total.astype(BF)
            for d in (1, 3, 2):
                to = turn(self.pos2, d)
                send(tosend.at[(*self.at, to)], torecv.at[(*self.at, d - 1)], self.dev2(d), self.on_2)

        def fourth(self, group):
            expect(self.on_2, torecv.at[self.at])
            branch = rsum[(*self.at, self.pos2)]
            for d in range(3):
                branch = branch + torecv[(*self.at, d)].astype(F32)
            part = slice(self.kind * 48, self.kind * 48 + 48)
            mixed = residual_scale * nloc[group, part].astype(F32) + branch
            mo[group, part] = mixed
            mob[y, places[self.k], part] = mixed.astype(BF)

    groups = [z, turn(z, -1), turn(z, 1), turn(z, 2)]
    places = [1, 0, 2, 3]
    reduces = [(Reduce(k, 0), Reduce(k, 1)) for k in range(4)]

    def first(k):
        down(k, groups[k])
        for one in reduces[k]:
            one.first()

    def second_(k):
        for one in reduces[k]:
            one.second()

    def third(k):
        for one in reduces[k]:
            one.third()

    def fourth(k):
        for one in reduces[k]:
            one.fourth(groups[k])

    first(0)
    hrings[0].forward()
    hrings[1].forward()
    second_(0)
    hrings[2].forward()
    third(0)
    hrings[3].forward()
    first(1)
    first(2)
    fourth(0)
    second_(1)
    second_(2)
    for ring in hrings:
        ring.finish()
    first(3)
    third(1)
    third(2)
    second_(3)
    fourth(1)
    fourth(2)
    third(3)

    def mblk(i, half):
        if half is None:
            return mob.at[i, pl.ds(0, 3)]
        return mob.at[i, pl.ds(0, 3), pl.ds(half * 48, 48)]

    ring = Ring(y, at_y, mblk)
    ring.start()
    fourth(3)
    stat = exchange_start(tx_s, sums_of([mo[i] for i in range(4)]), tx_r, at_x, 4)
    last = channel()
    for d in (1, 3, 2):
        send(mob.at[y, 3], mob.at[y, 3], at_y(d), last)
    ring.forward()
    totals[0] = exchange_end(stat, tx_s, tx_r)
    stat = channel()
    for d in range(1, 16):
        send(totals.at[0], totals.at[d], at_zy(d), stat)
    ring.finish()
    expect(last, mob.at[pl.ds(0, 3), 3])
    expect(stat, totals.at[pl.ds(1, 15)])
    columns = columns_of([totals[i] + totals[4 + i] + totals[8 + i] + totals[12 + i] for i in range(4)])
    for dy in range(4):
        yy = turn(y, -dy)
        for g in range(4):
            mean, scale = moments(columns, dy * 8 + g)
            block = (mob[yy, turn(1 - z, g)].astype(F32) - mean) * scale
            obuf[yy, g] = (block * go[...] + bo[...]).astype(BF)
            fetch(obuf.at[yy, g], out.at[g, yy], 4)
    assert len(used) == N_RECV, len(used)
    for copy in remote[-N_SEND:]:
        copy.wait_send()
    pltpu.make_async_copy(obuf, out, local_sem.at[4]).wait()


N_SEND = 64
N_RECV = 124
N_LOCAL = 5


def per_device(carried, branch_in, gain_in, bias_in, up_weight, down_weight, gain_out, bias_out):
    any_spec = pl.BlockSpec(memory_space=pl.ANY)
    vmem_spec = pl.BlockSpec(memory_space=pltpu.VMEM)
    V = pltpu.VMEM
    result = pl.pallas_call(
        kernel,
        out_shape=jax.ShapeDtypeStruct((4, 4, Q, W), BF),
        in_specs=[any_spec, any_spec, vmem_spec, vmem_spec, any_spec, any_spec, vmem_spec, vmem_spec],
        out_specs=any_spec,
        scratch_shapes=[
            V((4, Q, W), BF), V((4, Q, W), BF), V((4, Q, W), BF),
            V((G, D), BF), V((D, FS), BF), V((4, FS, W), BF), V((4, G, FS), BF),
            V((4, 4, 4, Q, W), F32), V((4, 4, 4, Q, W), BF),
            *[V((4, 2, 2, 48, W), BF) for _ in range(4)],
            V((4, 2, 4, 48, W), BF), V((4, 2, 4, 48, W), BF),
            V((4, 2, 4, 48, W), F32), V((4, 2, 4, 48, W), BF), V((4, 2, 3, 48, W), BF),
            V((4, Q, W), F32), V((4, 4, Q, W), BF), V((4, 4, Q, W), BF),
            V((8, 128), F32), V((15, 8, 128), F32),
            V((8, 128), F32), V((3, 8, 128), F32), V((16, 8, 128), F32),
            pltpu.SemaphoreType.DMA((N_SEND,)),
            pltpu.SemaphoreType.DMA((N_RECV,)),
            pltpu.SemaphoreType.DMA((N_LOCAL,)),
            pltpu.SemaphoreType.REGULAR,
        ],
        compiler_params=pltpu.CompilerParams(
            collective_id=0, has_side_effects=True, vmem_limit_bytes=60 * 1024 * 1024
        ),
    )(
        carried.reshape(4, 4, Q, W), branch_in.reshape(4, 4, Q, W),
        gain_in.reshape(1, W), bias_in.reshape(1, W), up_weight, down_weight,
        gain_out.reshape(1, W), bias_out.reshape(1, W),
    )
    return result.reshape(carried.shape)


def solution(mesh):
    in_specs = (
        P("dp", "ra"),
        P("dp", "ra"),
        P("ra"),
        P("ra"),
        P("ra", "cb"),
        P("cb", "ra"),
        P("ra"),
        P("ra"),
    )
    out_specs = P("dp", "ra")
    return jax.shard_map(
        per_device, mesh=mesh, in_specs=in_specs, out_specs=out_specs, check_vma=False
    )
```

```python
import functools

import jax
import jax.numpy as jnp
from jax import lax
from jax.experimental import pallas as pl
from jax.experimental.pallas import tpu as pltpu
from jax.sharding import PartitionSpec as P

residual_scale = 2.0**0.25
norm_eps = 1e-05
MESH = pl.DeviceIdType.MESH
BF = jnp.bfloat16
F32 = jnp.float32

Q = 96
G = 4 * Q
W = 256
D = 16 * W
FS = 1024


def kernel(
    car, bra, gi, bi, wu_in, wd_in, go, bo, out,
    cbuf, bbuf, nloc, nb, wu, wd, hid, pf, pb, opp_p, opp_m, sum_p, sum_m,
    from_m, from_p, direct, rsum, tosend, torecv, mo, mob, obuf,
    sx_s, sx_r, tx_s, tx_r, totals,
    send_sem, recv_sem, local_sem, hello, plane_x, plane_y,
):
    r = lax.axis_index("ra")
    y = lax.axis_index("cb")
    c = lax.axis_index("dp")
    z = lax.div(r, 4)
    x = lax.rem(r, 4)

    def turn(i, d):
        return lax.rem(i + d + 4, 4)

    def at_x(d):
        return (z * 4 + turn(x, d), y, c)

    def at_z(d):
        return (turn(z, d) * 4 + x, y, c)

    def at_y(d):
        return (r, turn(y, d), c)

    def at_zx(d):
        return (turn(z, d // 4) * 4 + turn(x, d % 4), y, c)

    def at_zy(d):
        return (turn(z, d // 4) * 4 + x, turn(y, d % 4), c)

    partner = (r, y, 1 - c)
    remote = []
    local = []

    used = []

    def channel():
        used.append(len(used))
        return used[-1]

    def described(src, dst, device, slot, on):
        return pltpu.make_async_remote_copy(
            src_ref=src, dst_ref=dst, send_sem=send_sem.at[slot], recv_sem=recv_sem.at[on],
            device_id=device, device_id_type=MESH,
        )

    def send(src, dst, device, on=None):
        k = len(remote)
        if k >= N_SEND:
            remote[k - N_SEND].wait_send()
        copy = described(src, dst, device, k % N_SEND, channel() if on is None else on)
        copy.start()
        remote.append(copy)
        return copy

    def expect(on, cover):
        described(cover, cover, partner, 0, on).wait_recv()

    def fetch(src, dst, on=None):
        k = len(local) if on is None else on
        copy = pltpu.make_async_copy(src, dst, local_sem.at[k])
        copy.start()
        local.append(copy)
        return copy

    class Ring:
        def __init__(self, pos, dev, blk):
            self.pos, self.dev, self.blk = pos, dev, blk

        def start(self):
            mine = self.blk(self.pos, None)
            self.p = send(mine, mine, self.dev(1))
            self.m = send(mine, mine, self.dev(-1))

        def forward(self):
            self.on = channel()
            self.p.wait_recv()
            half = self.blk(turn(self.pos, -1), 0)
            send(half, half, self.dev(1), self.on)
            self.m.wait_recv()
            half = self.blk(turn(self.pos, 1), 1)
            send(half, half, self.dev(-1), self.on)

        def finish(self):
            expect(self.on, self.blk(turn(self.pos, 2), None))

    def rows(start, size, step):
        return pl.ds(pl.multiple_of(start, step), size)

    load_c = fetch(car.at[:, y], cbuf)
    load_b = fetch(bra.at[:, y], bbuf)

    def wrow(zz, xx, cc):
        return (lax.div(zz, 2) * 4 + xx) * 512 + lax.rem(zz, 2) * 256 + cc * 128

    def wblk(zz, xx, f, half=None):
        start = wrow(zz, xx, c)
        if half is None:
            return wu.at[rows(start, 128, 128), pl.ds(f * 512, 512)]
        return wu.at[rows(start + half * 64, 64, 64), pl.ds(f * 512, 512)]

    load_wu = fetch(
        wu_in.at[rows(c * 128, 128, 128), rows(x * FS, FS, FS)],
        wu.at[rows(wrow(z, x, c), 128, 128), :],
    )
    wd_half = rows(c * 512, 512, 512)
    load_wd = fetch(wd_in.at[rows(x * FS + c * 512, 512, 512), :], wd.at[x, wd_half, :])

    barrier = pltpu.get_barrier_semaphore()
    friends = [dev(d) for dev in (at_x, at_z, at_y) for d in (1, 2, 3)]
    for device in friends:
        pl.semaphore_signal(barrier, inc=1, device_id=device, device_id_type=MESH)

    @pl.when(c == 0)
    def _():
        pl.semaphore_signal(barrier, inc=1, device_id=partner, device_id_type=MESH)

    def mixed_of(i):
        return residual_scale * cbuf[i].astype(F32) + bbuf[i].astype(F32)

    def sums_of(groups):
        lane = lax.broadcasted_iota(jnp.int32, (128, 128), 1)
        packed = jnp.zeros((128, 128), F32)
        pad = jnp.zeros((32, 1), F32)
        for g, mixed in enumerate(groups):
            total = jnp.sum(mixed, axis=1, keepdims=True)
            square = jnp.sum(mixed * mixed, axis=1, keepdims=True)
            packed = jnp.where(lane == g, jnp.concatenate([total, pad], axis=0), packed)
            packed = jnp.where(lane == 4 + g, jnp.concatenate([square, pad], axis=0), packed)
        return jnp.transpose(packed)[0:8]

    def columns_of(sums):
        return jnp.transpose(jnp.concatenate(sums + [sums[0]] * (16 - len(sums)), axis=0))[0:Q]

    def moments(columns, at):
        mean = columns[:, at : at + 1] / D
        var = columns[:, at + 4 : at + 5] / D - mean * mean
        return mean, lax.rsqrt(var + norm_eps)

    def exchange_start(buf, own, got, dev, n):
        buf[...] = own
        on = channel()
        for d in range(1, n):
            send(buf, got.at[d - 1], dev(d), on)
        return on

    def exchange_end(on, buf, got):
        expect(on, got)
        return sum((got[d] for d in range(got.shape[0])), buf[...])

    d2d = (channel(), channel())

    held = []

    def share(zz, xx, f):
        if held is None:
            send(wblk(zz, xx, f), wblk(zz, xx, f), partner, d2d[f])
        else:
            held.append((zz, xx, f))

    def share_held():
        nonlocal held

        @pl.when(c == 0)
        def _():
            pl.semaphore_wait(hello, 1)

        ready, held = held, None
        for one in ready:
            share(*one)

    def shared(f):
        expect(d2d[f], wu.at[pl.ds(0, D // 2), pl.ds(f * 512, 512)])

    def wring(u, f):
        xx = turn(x, -u)
        return Ring(z, at_z, lambda i, half: wblk(i, xx, f, half))

    wrings = {(u, f): wring(u, f) for u in range(4) for f in range(2)}
    a2a = {}

    def wu_send(d, f):
        cols = rows(turn(x, d) * FS + f * 512, 512, 512)
        a2a[d, f] = send(wu_in.at[rows(c * 128, 128, 128), cols], wblk(z, x, f), at_x(d))

    def w_start(u, f):
        if u:
            a2a[u, f].wait_recv()
        wrings[u, f].start()
        share(z, turn(x, -u), f)

    def w_forward(u, f):
        wrings[u, f].forward()
        share(turn(z, -1), turn(x, -u), f)
        share(turn(z, 1), turn(x, -u), f)

    def w_finish(u, f):
        wrings[u, f].finish()
        share(turn(z, 2), turn(x, -u), f)

    load_c.wait()
    load_b.wait()
    own_sums = sums_of([mixed_of(i) for i in range(4)])
    load_wu.wait()
    pl.semaphore_wait(barrier, len(friends) + c)

    @pl.when(c == 1)
    def _():
        pl.semaphore_signal(hello, inc=1, device_id=partner, device_id_type=MESH)

    for d in (1, 2, 3):
        pl.semaphore_signal(plane_x, inc=1, device_id=at_x(d), device_id_type=MESH)
        pl.semaphore_signal(plane_y, inc=1, device_id=at_y(d), device_id_type=MESH)
    pl.semaphore_wait(plane_x, 3)
    stat = exchange_start(sx_s, own_sums, sx_r, at_zx, 16)
    w_start(0, 0)
    for d in (1, 3, 2):
        wu_send(d, 0)
    w_start(0, 1)
    for d in (1, 3, 2):
        wu_send(d, 1)
    columns = columns_of([exchange_end(stat, sx_s, sx_r)])
    for i in range(4):
        mean, scale = moments(columns, i)
        nloc[i] = ((mixed_of(i) - mean) * scale * gi[...] + bi[...]).astype(BF)

    ncol = (lax.div(z, 2) * 4 + x) * 512 + lax.rem(z, 2) * 256
    mine = nb.at[rows(y * Q, Q, 32), rows(ncol, W, W)]
    nsend = channel()
    for d in (2, 1, 3):
        send(nloc.at[turn(z, d)], mine, at_z(d), nsend)
    nb[rows(y * Q, Q, 32), rows(ncol, W, W)] = nloc[z]
    w_forward(0, 0)
    w_start(1, 0)
    w_start(3, 0)
    expect(nsend, nloc.at[pl.ds(0, 3)])

    def nblk(h, xx, yy, part):
        col, size = h * 2048 + xx * 512, 512
        if part is not None:
            col, size = col + part * 256, 256
        return nb.at[rows(yy * Q, Q, 32), rows(col, size, 256)]

    a1 = Ring(x, at_x, lambda i, part: nblk(0, i, y, part))
    b1 = Ring(y, at_y, lambda i, part: nblk(1, x, i, part))

    def second(j):
        return (
            Ring(y, at_y, lambda i, part: nblk(0, turn(x, -j), i, part)),
            Ring(x, at_x, lambda i, part: nblk(1, i, turn(y, -j), part)),
        )

    seconds = [second(j) for j in range(4)]

    def n_start(j):
        for ring in seconds[j]:
            ring.start()

    def n_forward(j):
        for ring in seconds[j]:
            ring.forward()

    a1.start()
    b1.start()
    n_start(0)
    w_start(2, 0)
    b1.forward()
    a1.forward()
    n_start(1)
    n_start(3)
    w_forward(1, 0)
    share_held()
    n_forward(0)
    w_forward(3, 0)
    b1.finish()
    a1.finish()
    n_start(2)
    w_start(1, 1)
    w_forward(2, 0)
    w_start(3, 1)
    w_start(2, 1)
    w_forward(0, 1)
    n_forward(1)
    n_forward(3)
    n_forward(2)
    w_forward(1, 1)

    wd_a2a, wshare = channel(), channel()
    for d in (1, 3, 2):
        to = turn(x, d)
        part = wd_in.at[rows(to * FS + c * 512, 512, 512), :]
        send(part, wd.at[x, wd_half, :], at_x(d), wd_a2a)
    load_wd.wait()
    for u in (0, 1, 3, 2):
        w_finish(u, 0)
    for pair in seconds:
        for ring in pair:
            ring.finish()
    w_forward(3, 1)
    shared(0)

    hsent = []

    def up(n):
        cols = slice(n * 256, (n + 1) * 256)
        pre = sum(
            jnp.dot(nb[:, i : i + 1024], wu[i : i + 1024, cols], preferred_element_type=F32)
            for i in range(0, D, 1024)
        )
        hidden = jnp.square(jnp.maximum(pre, 0.0)).astype(BF)
        for i in range(4):
            hid[z, i, :, cols] = hidden[i * Q : (i + 1) * Q]

    def h_start(n):
        mine = hid.at[z, :, :, pl.ds(n * 256, 256)]
        hsent.append((send(mine, mine, at_z(1)), send(mine, mine, at_z(-1))))

    hon = (channel(), channel())

    def h_forward(n, late):
        for i, copy in enumerate(hsent[n]):
            if not late:
                copy.wait_recv()
            group = turn(z, 2 * i - 1)
            part = hid.at[group, pl.ds(2 * i, 2), pl.ds(48 * late, 48), pl.ds(n * 256, 256)]
            send(part, part, at_z(1 - 2 * i), hon[late])

    up(0)
    w_forward(2, 1)
    h_start(0)
    up(1)
    h_start(1)
    for u in (0, 1, 3, 2):
        w_finish(u, 1)
    shared(1)
    up(2)
    h_start(2)
    expect(wd_a2a, wd.at[pl.ds(0, 3), wd_half, :])
    send(wd.at[:, wd_half, :], wd.at[:, wd_half, :], partner, wshare)
    up(3)
    h_start(3)
    expect(wshare, wd.at[:, wd_half, :])

    def down(k, group, at):
        size = 4 * at.size
        lhs = hid[group, :, at].reshape(size, FS)
        for j in range(4):
            part = jnp.dot(lhs, wd[j], preferred_element_type=F32).reshape(4, at.size, W)
            for kind in range(2):
                lanes = slice(kind * 128, kind * 128 + 128)
                pf[k, kind, j, :, at] = part[:, :, lanes]
                pb[k, kind, j, :, at] = part[:, :, lanes].astype(BF)

    class Reduce:
        def __init__(self, k, kind, at):
            self.k, self.kind, self.rows = k, kind, at
            self.pos, self.dev = ((y, at_y), (x, at_x))[kind]
            self.pos2, self.dev2 = ((x, at_x), (y, at_y))[kind]

        def item(self, to, first, count):
            where = (pl.ds(first, count), to) if self.kind == 0 else (to, pl.ds(first, count))
            return (self.k, self.kind, *where, self.rows)

        def of(self, ref, *where):
            return (ref.at[(self.k, self.kind, *where, self.rows)])

        def first(self):
            self.on_m, self.on_2 = channel(), channel()
            if self.k == 3:
                for d in (2, 1, 3):
                    part = pb.at[self.item(turn(self.pos, d), 0, 4)]
                    send(part, direct.at[self.kind, d - 1, :, self.rows], self.dev(d), self.on_m)
                return
            self.on_p = channel()
            far, p, m = turn(self.pos, 2), turn(self.pos, 1), turn(self.pos, -1)
            self.p, self.m = p, m
            low, high = pl.ds(0, 2), pl.ds(2, 2)
            self.op = send(pb.at[self.item(far, 0, 2)], self.of(opp_p, slice(None)), self.dev(1))
            self.om = send(pb.at[self.item(far, 2, 2)], self.of(opp_m, slice(None)), self.dev(-1))
            send(pb.at[self.item(p, 2, 2)], self.of(from_m, high), self.dev(1), self.on_m)
            send(pb.at[self.item(m, 0, 2)], self.of(from_p, low), self.dev(-1), self.on_p)

        def second(self):
            at = (self.k, self.kind)
            self.op.wait_recv()
            sum_p[at] = (pf[self.item(self.p, 0, 2)] + opp_p[at].astype(F32)).astype(BF)
            send(sum_p.at[at], self.of(from_m, pl.ds(0, 2)), self.dev(1), self.on_m)
            self.om.wait_recv()
            sum_m[at] = (pf[self.item(self.m, 2, 2)] + opp_m[at].astype(F32)).astype(BF)
            send(sum_m.at[at], self.of(from_p, pl.ds(2, 2)), self.dev(-1), self.on_p)

        def third(self):
            total = pf[self.item(self.pos, 0, 4)]
            if self.k == 3:
                expect(self.on_m, direct.at[self.kind, :, :, self.rows])
                for d in range(3):
                    total = total + direct[self.kind, d, :, self.rows].astype(F32)
            else:
                at = (self.k, self.kind)
                expect(self.on_m, from_m.at[at])
                expect(self.on_p, from_p.at[at])
                total = total + from_m[at].astype(F32) + from_p[at].astype(F32)
            rsum[self.k, self.kind, :, self.rows] = total
            tosend[self.k, self.kind, :, self.rows] = total.astype(BF)
            for d in (1, 3, 2):
                to = turn(self.pos2, d)
                send(self.of(tosend, to), self.of(torecv, d - 1), self.dev2(d), self.on_2)

        def fourth(self, group):
            expect(self.on_2, self.of(torecv, slice(None)))
            branch = rsum[self.k, self.kind, self.pos2, self.rows]
            for d in range(3):
                branch = branch + torecv[self.k, self.kind, d, self.rows].astype(F32)
            lanes = slice(self.kind * 128, self.kind * 128 + 128)
            mixed = residual_scale * nloc[group, self.rows, lanes].astype(F32) + branch
            mo[group, self.rows, lanes] = mixed
            mob[y, places[self.k], self.rows, lanes] = mixed.astype(BF)

    groups = [z, turn(z, -1), turn(z, 1), turn(z, 2)]
    places = [1, 0, 2, 3]
    batches = [(0, pl.ds(0, Q)), (1, pl.ds(0, Q)), (2, pl.ds(0, Q)), (3, pl.ds(0, 48)), (3, pl.ds(48, 48))]
    reduces = [(Reduce(k, 0, at), Reduce(k, 1, at)) for k, at in batches]

    def first(b):
        k, at = batches[b]
        down(k, groups[k], at)
        for one in reduces[b]:
            one.first()

    def second_(b):
        for one in reduces[b]:
            one.second()

    def third(b):
        for one in reduces[b]:
            one.third()

    def fourth(b):
        for one in reduces[b]:
            one.fourth(groups[batches[b][0]])

    def h_finish(late):
        expect(hon[late], hid.at[0, :, pl.ds(0, 48), :])

    first(0)
    h_forward(0, 0)
    h_forward(1, 0)
    second_(0)
    h_forward(2, 0)
    third(0)
    h_forward(3, 0)
    for n in range(4):
        h_forward(n, 1)
    def gather(place):
        def mblk(i, half):
            if half is None:
                return mob.at[i, place]
            return mob.at[i, place, pl.ds(half * 48, 48)]

        ring = Ring(y, at_y, mblk)
        ring.start()
        return ring

    first(1)
    first(2)
    fourth(0)
    gathers = [gather(places[0])]
    second_(1)
    second_(2)
    h_finish(0)
    first(3)
    third(1)
    gathers[0].forward()
    h_finish(1)
    first(4)
    third(2)
    third(3)
    fourth(1)
    gathers.append(gather(places[1]))
    third(4)
    fourth(2)
    gathers.append(gather(places[2]))
    fourth(3)
    fourth(4)

    stat = exchange_start(tx_s, sums_of([mo[i] for i in range(4)]), tx_r, at_x, 4)
    last = channel()
    for d in (1, 3, 2):
        send(mob.at[y, 3], mob.at[y, 3], at_y(d), last)
    totals[0] = exchange_end(stat, tx_s, tx_r)
    stat = channel()
    pl.semaphore_wait(plane_y, 3)
    for d in range(1, 16):
        send(totals.at[0], totals.at[d], at_zy(d), stat)
    gathers[1].forward()
    gathers[2].forward()
    for ring in gathers:
        ring.finish()
    expect(last, mob.at[pl.ds(0, 3), 3])
    expect(stat, totals.at[pl.ds(1, 15)])
    columns = columns_of([totals[i] + totals[4 + i] + totals[8 + i] + totals[12 + i] for i in range(4)])
    for dy in range(4):
        yy = turn(y, -dy)
        for g in range(4):
            mean, scale = moments(columns, dy * 8 + g)
            block = (mob[yy, turn(1 - z, g)].astype(F32) - mean) * scale
            obuf[yy, g] = (block * go[...] + bo[...]).astype(BF)
            fetch(obuf.at[yy, g], out.at[g, yy], 4)
    assert len(used) == N_RECV, len(used)
    for copy in remote[-N_SEND:]:
        copy.wait_send()
    pltpu.make_async_copy(obuf, out, local_sem.at[4]).wait()


N_SEND = 64
N_RECV = 126
N_LOCAL = 5


def per_device(carried, branch_in, gain_in, bias_in, up_weight, down_weight, gain_out, bias_out):
    any_spec = pl.BlockSpec(memory_space=pl.ANY)
    vmem_spec = pl.BlockSpec(memory_space=pltpu.VMEM)
    V = pltpu.VMEM
    result = pl.pallas_call(
        kernel,
        out_shape=jax.ShapeDtypeStruct((4, 4, Q, W), BF),
        in_specs=[any_spec, any_spec, vmem_spec, vmem_spec, any_spec, any_spec, vmem_spec, vmem_spec],
        out_specs=any_spec,
        scratch_shapes=[
            V((4, Q, W), BF), V((4, Q, W), BF), V((4, Q, W), BF),
            V((G, D), BF), V((D, FS), BF), V((4, FS, W), BF), V((4, 4, Q, FS), BF),
            V((4, 2, 4, 4, Q, 128), F32), V((4, 2, 4, 4, Q, 128), BF),
            *[V((3, 2, 2, Q, 128), BF) for _ in range(4)],
            V((3, 2, 4, Q, 128), BF), V((3, 2, 4, Q, 128), BF), V((2, 3, 4, Q, 128), BF),
            V((4, 2, 4, Q, 128), F32), V((4, 2, 4, Q, 128), BF), V((4, 2, 3, Q, 128), BF),
            V((4, Q, W), F32), V((4, 4, Q, W), BF), V((4, 4, Q, W), BF),
            V((8, 128), F32), V((15, 8, 128), F32),
            V((8, 128), F32), V((3, 8, 128), F32), V((16, 8, 128), F32),
            pltpu.SemaphoreType.DMA((N_SEND,)),
            pltpu.SemaphoreType.DMA((N_RECV,)),
            pltpu.SemaphoreType.DMA((N_LOCAL,)),
            *[pltpu.SemaphoreType.REGULAR] * 3,
        ],
        compiler_params=pltpu.CompilerParams(
            collective_id=0, has_side_effects=True, vmem_limit_bytes=60 * 1024 * 1024
        ),
    )(
        carried.reshape(4, 4, Q, W), branch_in.reshape(4, 4, Q, W),
        gain_in.reshape(1, W), bias_in.reshape(1, W), up_weight, down_weight,
        gain_out.reshape(1, W), bias_out.reshape(1, W),
    )
    return result.reshape(carried.shape)


def solution(mesh):
    in_specs = (
        P("dp", "ra"),
        P("dp", "ra"),
        P("ra"),
        P("ra"),
        P("ra", "cb"),
        P("cb", "ra"),
        P("ra"),
        P("ra"),
    )
    out_specs = P("dp", "ra")
    return jax.shard_map(
        per_device, mesh=mesh, in_specs=in_specs, out_specs=out_specs, check_vma=False
    )
```

```python
import functools

import jax
import jax.numpy as jnp
from jax import lax
from jax.experimental import pallas as pl
from jax.experimental.pallas import tpu as pltpu
from jax.sharding import PartitionSpec as P

residual_scale = 2.0**0.25
norm_eps = 1e-05
MESH = pl.DeviceIdType.MESH
BF = jnp.bfloat16
F32 = jnp.float32

Q = 96
G = 4 * Q
W = 256
D = 16 * W
FS = 1024


def kernel(
    car, bra, gi, bi, wu_in, wd_in, go, bo, out,
    cbuf, bbuf, nloc, nb, wu, wd, hid, pf, pb, opp_p, opp_m, sum_p, sum_m,
    from_m, from_p, direct, rsum, tosend, torecv, mo, mob, obuf,
    sx_s, sx_r, tx_s, tx_r, totals,
    send_sem, recv_sem, local_sem, hello, plane_x, plane_y,
):
    r = lax.axis_index("ra")
    y = lax.axis_index("cb")
    c = lax.axis_index("dp")
    z = lax.div(r, 4)
    x = lax.rem(r, 4)

    def turn(i, d):
        return lax.rem(i + d + 4, 4)

    def at_x(d):
        return (z * 4 + turn(x, d), y, c)

    def at_z(d):
        return (turn(z, d) * 4 + x, y, c)

    def at_y(d):
        return (r, turn(y, d), c)

    def at_zx(d):
        return (turn(z, d // 4) * 4 + turn(x, d % 4), y, c)

    def at_zy(d):
        return (turn(z, d // 4) * 4 + x, turn(y, d % 4), c)

    partner = (r, y, 1 - c)
    remote = []
    local = []

    used = []

    def channel():
        used.append(len(used))
        return used[-1]

    def described(src, dst, device, slot, on):
        return pltpu.make_async_remote_copy(
            src_ref=src, dst_ref=dst, send_sem=send_sem.at[slot], recv_sem=recv_sem.at[on],
            device_id=device, device_id_type=MESH,
        )

    def send(src, dst, device, on=None):
        k = len(remote)
        if k >= N_SEND:
            remote[k - N_SEND].wait_send()
        copy = described(src, dst, device, k % N_SEND, channel() if on is None else on)
        copy.start()
        remote.append(copy)
        return copy

    def expect(on, cover):
        described(cover, cover, partner, 0, on).wait_recv()

    def fetch(src, dst, on=None):
        k = len(local) if on is None else on
        copy = pltpu.make_async_copy(src, dst, local_sem.at[k])
        copy.start()
        local.append(copy)
        return copy

    class Ring:
        def __init__(self, pos, dev, both, blk):
            self.pos, self.dev, self.both, self.blk = pos, dev, both, blk

        def start(self):
            self.to = channel()
            mine = self.blk(self.pos, None)
            send(mine, mine, self.dev(1), self.to)
            send(mine, mine, self.dev(-1), self.to)

        def forward(self):
            self.on = channel()
            expect(self.to, self.both)
            for i in range(2):
                half = self.blk(turn(self.pos, 2 * i - 1), i)
                send(half, half, self.dev(1 - 2 * i), self.on)

        def finish(self):
            expect(self.on, self.blk(turn(self.pos, 2), None))

    def rows(start, size, step):
        return pl.ds(pl.multiple_of(start, step), size)

    load_c = fetch(car.at[:, y], cbuf)
    load_b = fetch(bra.at[:, y], bbuf)

    def wrow(zz, xx, cc):
        return (lax.div(zz, 2) * 4 + xx) * 512 + lax.rem(zz, 2) * 256 + cc * 128

    def wblk(zz, xx, f, half=None):
        start = wrow(zz, xx, c)
        if half is None:
            return wu.at[rows(start, 128, 128), pl.ds(f * 512, 512)]
        return wu.at[rows(start + half * 64, 64, 64), pl.ds(f * 512, 512)]

    load_wu = fetch(
        wu_in.at[rows(c * 128, 128, 128), rows(x * FS, FS, FS)],
        wu.at[rows(wrow(z, x, c), 128, 128), :],
    )
    wd_half = rows(c * 512, 512, 512)
    load_wd = fetch(wd_in.at[rows(x * FS + c * 512, 512, 512), :], wd.at[x, wd_half, :])

    barrier = pltpu.get_barrier_semaphore()
    friends = [dev(d) for dev in (at_x, at_z, at_y) for d in (1, 2, 3)]
    for device in friends:
        pl.semaphore_signal(barrier, inc=1, device_id=device, device_id_type=MESH)

    @pl.when(c == 0)
    def _():
        pl.semaphore_signal(barrier, inc=1, device_id=partner, device_id_type=MESH)

    def mixed_of(i):
        return residual_scale * cbuf[i].astype(F32) + bbuf[i].astype(F32)

    def sums_of(groups):
        lane = lax.broadcasted_iota(jnp.int32, (128, 128), 1)
        packed = jnp.zeros((128, 128), F32)
        pad = jnp.zeros((32, 1), F32)
        for g, mixed in enumerate(groups):
            total = jnp.sum(mixed, axis=1, keepdims=True)
            square = jnp.sum(mixed * mixed, axis=1, keepdims=True)
            packed = jnp.where(lane == g, jnp.concatenate([total, pad], axis=0), packed)
            packed = jnp.where(lane == 4 + g, jnp.concatenate([square, pad], axis=0), packed)
        return jnp.transpose(packed)[0:8]

    def columns_of(sums):
        return jnp.transpose(jnp.concatenate(sums + [sums[0]] * (16 - len(sums)), axis=0))[0:Q]

    def moments(columns, at):
        mean = columns[:, at : at + 1] / D
        var = columns[:, at + 4 : at + 5] / D - mean * mean
        return mean, lax.rsqrt(var + norm_eps)

    def exchange_start(buf, own, got, dev, n):
        buf[...] = own
        on = channel()
        for d in range(1, n):
            send(buf, got.at[d - 1], dev(d), on)
        return on

    def exchange_end(on, buf, got):
        expect(on, got)
        return sum((got[d] for d in range(got.shape[0])), buf[...])

    d2d = (channel(), channel())

    held = []

    def share(zz, xx, f):
        if held is None:
            send(wblk(zz, xx, f), wblk(zz, xx, f), partner, d2d[f])
        else:
            held.append((zz, xx, f))

    def share_held():
        nonlocal held

        @pl.when(c == 0)
        def _():
            pl.semaphore_wait(hello, 1)

        ready, held = held, None
        for one in ready:
            share(*one)

    def shared(f):
        expect(d2d[f], wu.at[pl.ds(0, D // 2), pl.ds(f * 512, 512)])

    def wring(u, f):
        xx = turn(x, -u)
        return Ring(z, at_z, wu.at[pl.ds(0, 256), pl.ds(0, 512)], lambda i, half: wblk(i, xx, f, half))

    wrings = {(u, f): wring(u, f) for u in range(4) for f in range(2)}
    a2a = {}

    def wu_send(d, f):
        cols = rows(turn(x, d) * FS + f * 512, 512, 512)
        a2a[d, f] = send(wu_in.at[rows(c * 128, 128, 128), cols], wblk(z, x, f), at_x(d))

    def w_start(u, f):
        if u:
            a2a[u, f].wait_recv()
        wrings[u, f].start()
        share(z, turn(x, -u), f)

    def w_forward(u, f):
        wrings[u, f].forward()
        share(turn(z, -1), turn(x, -u), f)
        share(turn(z, 1), turn(x, -u), f)

    def w_finish(u, f):
        wrings[u, f].finish()
        share(turn(z, 2), turn(x, -u), f)

    load_c.wait()
    load_b.wait()
    own_sums = sums_of([mixed_of(i) for i in range(4)])
    load_wu.wait()
    pl.semaphore_wait(barrier, len(friends) + c)

    @pl.when(c == 1)
    def _():
        pl.semaphore_signal(hello, inc=1, device_id=partner, device_id_type=MESH)

    for d in (1, 2, 3):
        pl.semaphore_signal(plane_x, inc=1, device_id=at_x(d), device_id_type=MESH)
        pl.semaphore_signal(plane_y, inc=1, device_id=at_y(d), device_id_type=MESH)
    w_start(0, 0)
    pl.semaphore_wait(plane_x, 3)
    stat = exchange_start(sx_s, own_sums, sx_r, at_zx, 16)
    for d in (1, 3, 2):
        wu_send(d, 0)
    w_start(0, 1)
    for d in (1, 3, 2):
        wu_send(d, 1)
    columns = columns_of([exchange_end(stat, sx_s, sx_r)])
    for i in range(4):
        mean, scale = moments(columns, i)
        nloc[i] = ((mixed_of(i) - mean) * scale * gi[...] + bi[...]).astype(BF)

    ncol = (lax.div(z, 2) * 4 + x) * 512 + lax.rem(z, 2) * 256
    mine = nb.at[rows(y * Q, Q, 32), rows(ncol, W, W)]
    nsend = channel()
    for d in (2, 1, 3):
        send(nloc.at[turn(z, d)], mine, at_z(d), nsend)
    nb[rows(y * Q, Q, 32), rows(ncol, W, W)] = nloc[z]
    w_forward(0, 0)
    w_start(1, 0)
    w_start(3, 0)
    expect(nsend, nloc.at[pl.ds(0, 3)])

    def nblk(h, xx, yy, part):
        col, size = h * 2048 + xx * 512, 512
        if part is not None:
            col, size = col + part * 256, 256
        return nb.at[rows(yy * Q, Q, 32), rows(col, size, 256)]

    two = nb.at[pl.ds(0, 2 * Q), pl.ds(0, 512)]
    a1 = Ring(x, at_x, two, lambda i, part: nblk(0, i, y, part))
    b1 = Ring(y, at_y, two, lambda i, part: nblk(1, x, i, part))

    def second(j):
        return (
            Ring(y, at_y, two, lambda i, part: nblk(0, turn(x, -j), i, part)),
            Ring(x, at_x, two, lambda i, part: nblk(1, i, turn(y, -j), part)),
        )

    seconds = [second(j) for j in range(4)]

    def n_start(j):
        for ring in seconds[j]:
            ring.start()

    def n_forward(j):
        for ring in seconds[j]:
            ring.forward()

    a1.start()
    b1.start()
    n_start(0)
    w_start(2, 0)
    b1.forward()
    a1.forward()
    n_start(1)
    n_start(3)
    w_forward(1, 0)
    share_held()
    n_forward(0)
    w_forward(3, 0)
    b1.finish()
    a1.finish()
    n_start(2)
    w_start(1, 1)
    w_forward(2, 0)
    w_start(3, 1)
    w_start(2, 1)
    w_forward(0, 1)
    n_forward(1)
    n_forward(3)
    n_forward(2)
    w_forward(1, 1)

    wd_a2a, wshare = channel(), channel()
    for d in (1, 3, 2):
        to = turn(x, d)
        part = wd_in.at[rows(to * FS + c * 512, 512, 512), :]
        send(part, wd.at[x, wd_half, :], at_x(d), wd_a2a)
    load_wd.wait()
    for u in (0, 1, 3, 2):
        w_finish(u, 0)
    for pair in seconds:
        for ring in pair:
            ring.finish()
    w_forward(3, 1)
    shared(0)

    hsent = []

    def up(n):
        cols = slice(n * 256, (n + 1) * 256)
        pre = sum(
            jnp.dot(nb[:, i : i + 1024], wu[i : i + 1024, cols], preferred_element_type=F32)
            for i in range(0, D, 1024)
        )
        hidden = jnp.square(jnp.maximum(pre, 0.0)).astype(BF)
        for i in range(4):
            hid[z, i, :, cols] = hidden[i * Q : (i + 1) * Q]

    def h_start(n):
        mine = hid.at[z, :, :, pl.ds(n * 256, 256)]
        hsent.append((send(mine, mine, at_z(1)), send(mine, mine, at_z(-1))))

    hon = (channel(), channel())

    def h_forward(n, late):
        for i, copy in enumerate(hsent[n]):
            if not late:
                copy.wait_recv()
            group = turn(z, 2 * i - 1)
            part = hid.at[group, pl.ds(2 * i, 2), pl.ds(48 * late, 48), pl.ds(n * 256, 256)]
            send(part, part, at_z(1 - 2 * i), hon[late])

    up(0)
    w_forward(2, 1)
    h_start(0)
    up(1)
    h_start(1)
    for u in (0, 1, 3, 2):
        w_finish(u, 1)
    shared(1)
    up(2)
    h_start(2)
    expect(wd_a2a, wd.at[pl.ds(0, 3), wd_half, :])
    send(wd.at[:, wd_half, :], wd.at[:, wd_half, :], partner, wshare)
    up(3)
    h_start(3)
    expect(wshare, wd.at[:, wd_half, :])

    def down(k, group, at):
        size = 4 * at.size
        lhs = hid[group, :, at].reshape(size, FS)
        for j in range(4):
            part = jnp.dot(lhs, wd[j], preferred_element_type=F32).reshape(4, at.size, W)
            for kind in range(2):
                lanes = slice(kind * 128, kind * 128 + 128)
                pf[k, kind, j, :, at] = part[:, :, lanes]
                pb[k, kind, j, :, at] = part[:, :, lanes].astype(BF)

    class Reduce:
        def __init__(self, k, kind, at):
            self.k, self.kind, self.rows = k, kind, at
            self.pos, self.dev = ((y, at_y), (x, at_x))[kind]
            self.pos2, self.dev2 = ((x, at_x), (y, at_y))[kind]

        def item(self, to, first, count):
            where = (pl.ds(first, count), to) if self.kind == 0 else (to, pl.ds(first, count))
            return (self.k, self.kind, *where, self.rows)

        def of(self, ref, *where):
            return (ref.at[(self.k, self.kind, *where, self.rows)])

        def first(self):
            self.on_m, self.on_2 = channel(), channel()
            if self.k == 3:
                for d in (2, 1, 3):
                    part = pb.at[self.item(turn(self.pos, d), 0, 4)]
                    send(part, direct.at[self.kind, d - 1, :, self.rows], self.dev(d), self.on_m)
                return
            self.on_p = channel()
            far, p, m = turn(self.pos, 2), turn(self.pos, 1), turn(self.pos, -1)
            self.p, self.m = p, m
            low, high = pl.ds(0, 2), pl.ds(2, 2)
            self.op = send(pb.at[self.item(far, 0, 2)], self.of(opp_p, slice(None)), self.dev(1))
            self.om = send(pb.at[self.item(far, 2, 2)], self.of(opp_m, slice(None)), self.dev(-1))
            send(pb.at[self.item(p, 2, 2)], self.of(from_m, high), self.dev(1), self.on_m)
            send(pb.at[self.item(m, 0, 2)], self.of(from_p, low), self.dev(-1), self.on_p)

        def second(self):
            at = (self.k, self.kind)
            self.op.wait_recv()
            sum_p[at] = (pf[self.item(self.p, 0, 2)] + opp_p[at].astype(F32)).astype(BF)
            send(sum_p.at[at], self.of(from_m, pl.ds(0, 2)), self.dev(1), self.on_m)
            self.om.wait_recv()
            sum_m[at] = (pf[self.item(self.m, 2, 2)] + opp_m[at].astype(F32)).astype(BF)
            send(sum_m.at[at], self.of(from_p, pl.ds(2, 2)), self.dev(-1), self.on_p)

        def third(self):
            total = pf[self.item(self.pos, 0, 4)]
            if self.k == 3:
                expect(self.on_m, direct.at[self.kind, :, :, self.rows])
                for d in range(3):
                    total = total + direct[self.kind, d, :, self.rows].astype(F32)
            else:
                at = (self.k, self.kind)
                expect(self.on_m, from_m.at[at])
                expect(self.on_p, from_p.at[at])
                total = total + from_m[at].astype(F32) + from_p[at].astype(F32)
            rsum[self.k, self.kind, :, self.rows] = total
            tosend[self.k, self.kind, :, self.rows] = total.astype(BF)
            for d in (1, 3, 2):
                to = turn(self.pos2, d)
                send(self.of(tosend, to), self.of(torecv, d - 1), self.dev2(d), self.on_2)

        def fourth(self, group):
            expect(self.on_2, self.of(torecv, slice(None)))
            branch = rsum[self.k, self.kind, self.pos2, self.rows]
            for d in range(3):
                branch = branch + torecv[self.k, self.kind, d, self.rows].astype(F32)
            lanes = slice(self.kind * 128, self.kind * 128 + 128)
            mixed = residual_scale * nloc[group, self.rows, lanes].astype(F32) + branch
            mo[group, self.rows, lanes] = mixed
            mob[y, places[self.k], self.rows, lanes] = mixed.astype(BF)

    groups = [z, turn(z, -1), turn(z, 1), turn(z, 2)]
    places = [1, 0, 2, 3]
    batches = [(0, pl.ds(0, Q)), (1, pl.ds(0, Q)), (2, pl.ds(0, Q)), (3, pl.ds(0, 48)), (3, pl.ds(48, 48))]
    reduces = [(Reduce(k, 0, at), Reduce(k, 1, at)) for k, at in batches]

    def first(b):
        k, at = batches[b]
        down(k, groups[k], at)
        for one in reduces[b]:
            one.first()

    def second_(b):
        for one in reduces[b]:
            one.second()

    def third(b):
        for one in reduces[b]:
            one.third()

    def fourth(b):
        for one in reduces[b]:
            one.fourth(groups[batches[b][0]])

    def h_finish(late):
        expect(hon[late], hid.at[0, :, pl.ds(0, 48), :])

    first(0)
    h_forward(0, 0)
    h_forward(1, 0)
    second_(0)
    h_forward(2, 0)
    third(0)
    h_forward(3, 0)
    for n in range(4):
        h_forward(n, 1)
    def gather(place):
        def mblk(i, half):
            if half is None:
                return mob.at[i, place]
            return mob.at[i, place, pl.ds(half * 48, 48)]

        ring = Ring(y, at_y, mob.at[pl.ds(0, 2), 0], mblk)
        ring.start()
        return ring

    first(1)
    first(2)
    fourth(0)
    gathers = [gather(places[0])]
    second_(1)
    h_finish(0)
    first(3)
    second_(2)
    h_finish(1)
    first(4)
    third(1)
    gathers[0].forward()
    third(2)
    third(3)
    fourth(1)
    gathers.append(gather(places[1]))
    third(4)
    fourth(2)
    gathers.append(gather(places[2]))
    fourth(3)
    fourth(4)

    stat = exchange_start(tx_s, sums_of([mo[i] for i in range(4)]), tx_r, at_x, 4)
    last = channel()
    for d in (1, 3, 2):
        send(mob.at[y, 3], mob.at[y, 3], at_y(d), last)
    totals[0] = exchange_end(stat, tx_s, tx_r)
    stat = channel()
    pl.semaphore_wait(plane_y, 3)
    for d in range(1, 16):
        send(totals.at[0], totals.at[d], at_zy(d), stat)
    gathers[1].forward()
    gathers[2].forward()
    for ring in gathers:
        ring.finish()
    expect(last, mob.at[pl.ds(0, 3), 3])
    expect(stat, totals.at[pl.ds(1, 15)])
    columns = columns_of([totals[i] + totals[4 + i] + totals[8 + i] + totals[12 + i] for i in range(4)])
    for dy in range(4):
        yy = turn(y, -dy)
        for g in range(4):
            mean, scale = moments(columns, dy * 8 + g)
            block = (mob[yy, turn(1 - z, g)].astype(F32) - mean) * scale
            obuf[yy, g] = (block * go[...] + bo[...]).astype(BF)
            fetch(obuf.at[yy, g], out.at[g, yy], 4)
    assert len(used) == N_RECV, len(used)
    for copy in remote[-N_SEND:]:
        copy.wait_send()
    pltpu.make_async_copy(obuf, out, local_sem.at[4]).wait()


N_SEND = 40
N_RECV = 105
N_LOCAL = 5


def per_device(carried, branch_in, gain_in, bias_in, up_weight, down_weight, gain_out, bias_out):
    any_spec = pl.BlockSpec(memory_space=pl.ANY)
    vmem_spec = pl.BlockSpec(memory_space=pltpu.VMEM)
    V = pltpu.VMEM
    result = pl.pallas_call(
        kernel,
        out_shape=jax.ShapeDtypeStruct((4, 4, Q, W), BF),
        in_specs=[any_spec, any_spec, vmem_spec, vmem_spec, any_spec, any_spec, vmem_spec, vmem_spec],
        out_specs=any_spec,
        scratch_shapes=[
            V((4, Q, W), BF), V((4, Q, W), BF), V((4, Q, W), BF),
            V((G, D), BF), V((D, FS), BF), V((4, FS, W), BF), V((4, 4, Q, FS), BF),
            V((4, 2, 4, 4, Q, 128), F32), V((4, 2, 4, 4, Q, 128), BF),
            *[V((3, 2, 2, Q, 128), BF) for _ in range(4)],
            V((3, 2, 4, Q, 128), BF), V((3, 2, 4, Q, 128), BF), V((2, 3, 4, Q, 128), BF),
            V((4, 2, 4, Q, 128), F32), V((4, 2, 4, Q, 128), BF), V((4, 2, 3, Q, 128), BF),
            V((4, Q, W), F32), V((4, 4, Q, W), BF), V((4, 4, Q, W), BF),
            V((8, 128), F32), V((15, 8, 128), F32),
            V((8, 128), F32), V((3, 8, 128), F32), V((16, 8, 128), F32),
            pltpu.SemaphoreType.DMA((N_SEND,)),
            pltpu.SemaphoreType.DMA((N_RECV,)),
            pltpu.SemaphoreType.DMA((N_LOCAL,)),
            *[pltpu.SemaphoreType.REGULAR] * 3,
        ],
        compiler_params=pltpu.CompilerParams(
            collective_id=0, has_side_effects=True, vmem_limit_bytes=60 * 1024 * 1024
        ),
    )(
        carried.reshape(4, 4, Q, W), branch_in.reshape(4, 4, Q, W),
        gain_in.reshape(1, W), bias_in.reshape(1, W), up_weight, down_weight,
        gain_out.reshape(1, W), bias_out.reshape(1, W),
    )
    return result.reshape(carried.shape)


def solution(mesh):
    in_specs = (
        P("dp", "ra"),
        P("dp", "ra"),
        P("ra"),
        P("ra"),
        P("ra", "cb"),
        P("cb", "ra"),
        P("ra"),
        P("ra"),
    )
    out_specs = P("dp", "ra")
    return jax.shard_map(
        per_device, mesh=mesh, in_specs=in_specs, out_specs=out_specs, check_vma=False
    )
```

```python
import functools

import jax
import jax.numpy as jnp
from jax import lax
from jax.experimental import pallas as pl
from jax.experimental.pallas import tpu as pltpu
from jax.sharding import PartitionSpec as P

residual_scale = 2.0**0.25
norm_eps = 1e-05
MESH = pl.DeviceIdType.MESH
BF = jnp.bfloat16
F32 = jnp.float32

Q = 96
G = 4 * Q
W = 256
D = 16 * W
FS = 1024


def kernel(
    car, bra, gi, bi, wu_in, wd_in, go, bo, out,
    cbuf, bbuf, nloc, nb, wu, wd, hid, pf, pb, opp_p, opp_m, sum_p, sum_m,
    from_m, from_p, direct, rsum, tosend, torecv, mo, mob, obuf,
    sx_s, sx_r, tx_s, tx_r, totals,
    send_sem, recv_sem, local_sem, hello, plane_x, plane_y,
):
    r = lax.axis_index("ra")
    y = lax.axis_index("cb")
    c = lax.axis_index("dp")
    z = lax.div(r, 4)
    x = lax.rem(r, 4)

    def turn(i, d):
        return lax.rem(i + d + 4, 4)

    def at_x(d):
        return (z * 4 + turn(x, d), y, c)

    def at_z(d):
        return (turn(z, d) * 4 + x, y, c)

    def at_y(d):
        return (r, turn(y, d), c)

    def at_zx(d):
        return (turn(z, d // 4) * 4 + turn(x, d % 4), y, c)

    def at_zy(d):
        return (turn(z, d // 4) * 4 + x, turn(y, d % 4), c)

    partner = (r, y, 1 - c)
    remote = []
    local = []

    used = []

    def channel():
        used.append(len(used))
        return used[-1]

    def described(src, dst, device, slot, on):
        return pltpu.make_async_remote_copy(
            src_ref=src, dst_ref=dst, send_sem=send_sem.at[slot], recv_sem=recv_sem.at[on],
            device_id=device, device_id_type=MESH,
        )

    def send(src, dst, device, on=None):
        k = len(remote)
        if k >= N_SEND:
            remote[k - N_SEND].wait_send()
        copy = described(src, dst, device, k % N_SEND, channel() if on is None else on)
        copy.start()
        remote.append(copy)
        return copy

    def expect(on, cover):
        described(cover, cover, partner, 0, on).wait_recv()

    def fetch(src, dst, on=None):
        k = len(local) if on is None else on
        copy = pltpu.make_async_copy(src, dst, local_sem.at[k])
        copy.start()
        local.append(copy)
        return copy

    class Ring:
        def __init__(self, pos, dev, both, blk):
            self.pos, self.dev, self.both, self.blk = pos, dev, both, blk

        def start(self):
            self.to = channel()
            mine = self.blk(self.pos, None)
            send(mine, mine, self.dev(1), self.to)
            send(mine, mine, self.dev(-1), self.to)

        def forward(self):
            self.on = channel()
            expect(self.to, self.both)
            for i in range(2):
                half = self.blk(turn(self.pos, 2 * i - 1), i)
                send(half, half, self.dev(1 - 2 * i), self.on)

        def finish(self):
            expect(self.on, self.blk(turn(self.pos, 2), None))

    def rows(start, size, step):
        return pl.ds(pl.multiple_of(start, step), size)

    load_c = fetch(car.at[:, y], cbuf)
    load_b = fetch(bra.at[:, y], bbuf)

    def wrow(zz, xx, cc):
        return (lax.div(zz, 2) * 4 + xx) * 512 + lax.rem(zz, 2) * 256 + cc * 128

    def wblk(zz, xx, f, half=None):
        start = wrow(zz, xx, c)
        if half is None:
            return wu.at[rows(start, 128, 128), pl.ds(f * 512, 512)]
        return wu.at[rows(start + half * 64, 64, 64), pl.ds(f * 512, 512)]

    load_wu = fetch(
        wu_in.at[rows(c * 128, 128, 128), rows(x * FS, FS, FS)],
        wu.at[rows(wrow(z, x, c), 128, 128), :],
    )
    wd_half = rows(c * 512, 512, 512)
    load_wd = fetch(wd_in.at[rows(x * FS + c * 512, 512, 512), :], wd.at[x, wd_half, :])

    barrier = pltpu.get_barrier_semaphore()
    friends = [dev(d) for dev in (at_x, at_z, at_y) for d in (1, 2, 3)]
    for device in friends:
        pl.semaphore_signal(barrier, inc=1, device_id=device, device_id_type=MESH)

    @pl.when(c == 0)
    def _():
        pl.semaphore_signal(barrier, inc=1, device_id=partner, device_id_type=MESH)

    def mixed_of(i):
        return residual_scale * cbuf[i].astype(F32) + bbuf[i].astype(F32)

    def sums_of(groups):
        lane = lax.broadcasted_iota(jnp.int32, (128, 128), 1)
        packed = jnp.zeros((128, 128), F32)
        pad = jnp.zeros((32, 1), F32)
        for g, mixed in enumerate(groups):
            total = jnp.sum(mixed, axis=1, keepdims=True)
            square = jnp.sum(mixed * mixed, axis=1, keepdims=True)
            packed = jnp.where(lane == g, jnp.concatenate([total, pad], axis=0), packed)
            packed = jnp.where(lane == 4 + g, jnp.concatenate([square, pad], axis=0), packed)
        return jnp.transpose(packed)[0:8]

    def columns_of(sums):
        return jnp.transpose(jnp.concatenate(sums + [sums[0]] * (16 - len(sums)), axis=0))[0:Q]

    def moments(columns, at):
        mean = columns[:, at : at + 1] / D
        var = columns[:, at + 4 : at + 5] / D - mean * mean
        return mean, lax.rsqrt(var + norm_eps)

    def exchange_start(buf, own, got, dev, n):
        buf[...] = own
        on = channel()
        for d in range(1, n):
            send(buf, got.at[d - 1], dev(d), on)
        return on

    def exchange_end(on, buf, got):
        expect(on, got)
        return sum((got[d] for d in range(got.shape[0])), buf[...])

    d2d = (channel(), channel())

    held = []

    def share(zz, xx, f):
        if held is None:
            send(wblk(zz, xx, f), wblk(zz, xx, f), partner, d2d[f])
        else:
            held.append((zz, xx, f))

    def share_held():
        nonlocal held

        @pl.when(c == 0)
        def _():
            pl.semaphore_wait(hello, 1)

        ready, held = held, None
        for one in ready:
            share(*one)

    def shared(f):
        expect(d2d[f], wu.at[pl.ds(0, D // 2), pl.ds(f * 512, 512)])

    def wring(u, f):
        xx = turn(x, -u)
        return Ring(z, at_z, wu.at[pl.ds(0, 256), pl.ds(0, 512)], lambda i, half: wblk(i, xx, f, half))

    wrings = {(u, f): wring(u, f) for u in range(4) for f in range(2)}
    a2a = {}

    def wu_send(d, f):
        cols = rows(turn(x, d) * FS + f * 512, 512, 512)
        a2a[d, f] = send(wu_in.at[rows(c * 128, 128, 128), cols], wblk(z, x, f), at_x(d))

    def w_start(u, f):
        if u:
            a2a[u, f].wait_recv()
        wrings[u, f].start()
        share(z, turn(x, -u), f)

    def w_forward(u, f):
        wrings[u, f].forward()
        share(turn(z, -1), turn(x, -u), f)
        share(turn(z, 1), turn(x, -u), f)

    def w_finish(u, f):
        wrings[u, f].finish()
        share(turn(z, 2), turn(x, -u), f)

    load_c.wait()
    load_b.wait()
    own_sums = sums_of([mixed_of(i) for i in range(4)])
    load_wu.wait()
    pl.semaphore_wait(barrier, len(friends) + c)

    @pl.when(c == 1)
    def _():
        pl.semaphore_signal(hello, inc=1, device_id=partner, device_id_type=MESH)

    for d in (1, 2, 3):
        pl.semaphore_signal(plane_x, inc=1, device_id=at_x(d), device_id_type=MESH)
        pl.semaphore_signal(plane_y, inc=1, device_id=at_y(d), device_id_type=MESH)
    w_start(0, 0)
    pl.semaphore_wait(plane_x, 3)
    stat = exchange_start(sx_s, own_sums, sx_r, at_zx, 16)
    for d in (1, 3, 2):
        wu_send(d, 0)
    w_start(0, 1)
    for d in (1, 3, 2):
        wu_send(d, 1)
    columns = columns_of([exchange_end(stat, sx_s, sx_r)])
    for i in range(4):
        mean, scale = moments(columns, i)
        nloc[i] = ((mixed_of(i) - mean) * scale * gi[...] + bi[...]).astype(BF)

    ncol = (lax.div(z, 2) * 4 + x) * 512 + lax.rem(z, 2) * 256
    mine = nb.at[rows(y * Q, Q, 32), rows(ncol, W, W)]
    nsend = channel()
    for d in (2, 1, 3):
        send(nloc.at[turn(z, d)], mine, at_z(d), nsend)
    nb[rows(y * Q, Q, 32), rows(ncol, W, W)] = nloc[z]
    w_forward(0, 0)
    w_start(1, 0)
    w_start(3, 0)
    expect(nsend, nloc.at[pl.ds(0, 3)])

    def nblk(h, xx, yy, part):
        col, size = h * 2048 + xx * 512, 512
        if part is not None:
            col, size = col + part * 256, 256
        return nb.at[rows(yy * Q, Q, 32), rows(col, size, 256)]

    two = nb.at[pl.ds(0, 2 * Q), pl.ds(0, 512)]
    a1 = Ring(x, at_x, two, lambda i, part: nblk(0, i, y, part))
    b1 = Ring(y, at_y, two, lambda i, part: nblk(1, x, i, part))

    def second(j):
        return (
            Ring(y, at_y, two, lambda i, part: nblk(0, turn(x, -j), i, part)),
            Ring(x, at_x, two, lambda i, part: nblk(1, i, turn(y, -j), part)),
        )

    seconds = [second(j) for j in range(4)]

    def n_start(j):
        for ring in seconds[j]:
            ring.start()

    def n_forward(j):
        for ring in seconds[j]:
            ring.forward()

    a1.start()
    b1.start()
    n_start(0)
    w_start(2, 0)
    b1.forward()
    a1.forward()
    n_start(1)
    n_start(3)
    w_forward(1, 0)
    share_held()
    n_forward(0)
    w_forward(3, 0)
    b1.finish()
    a1.finish()
    n_start(2)
    w_start(1, 1)
    w_forward(2, 0)
    w_start(3, 1)
    w_start(2, 1)
    w_forward(0, 1)
    n_forward(1)
    n_forward(3)
    n_forward(2)
    w_forward(1, 1)

    wd_a2a, wshare = channel(), channel()
    for d in (1, 3, 2):
        to = turn(x, d)
        part = wd_in.at[rows(to * FS + c * 512, 512, 512), :]
        send(part, wd.at[x, wd_half, :], at_x(d), wd_a2a)
    load_wd.wait()
    for u in (0, 1, 3, 2):
        w_finish(u, 0)
    for pair in seconds:
        for ring in pair:
            ring.finish()
    w_forward(3, 1)
    shared(0)

    hsent = []

    def up(n):
        cols = slice(n * 256, (n + 1) * 256)
        pre = sum(
            jnp.dot(nb[:, i : i + 1024], wu[i : i + 1024, cols], preferred_element_type=F32)
            for i in range(0, D, 1024)
        )
        hidden = jnp.square(jnp.maximum(pre, 0.0)).astype(BF)
        for i in range(4):
            hid[z, i, :, cols] = hidden[i * Q : (i + 1) * Q]

    def h_start(n):
        mine = hid.at[z, :, :, pl.ds(n * 256, 256)]
        hsent.append((send(mine, mine, at_z(1)), send(mine, mine, at_z(-1))))

    hon = (channel(), channel())

    def h_forward(n, late):
        for i, copy in enumerate(hsent[n]):
            if not late:
                copy.wait_recv()
            group = turn(z, 2 * i - 1)
            part = hid.at[group, pl.ds(2 * i, 2), pl.ds(48 * late, 48), pl.ds(n * 256, 256)]
            send(part, part, at_z(1 - 2 * i), hon[late])

    up(0)
    w_forward(2, 1)
    h_start(0)
    up(1)
    h_start(1)
    for u in (0, 1, 3, 2):
        w_finish(u, 1)
    shared(1)
    up(2)
    h_start(2)
    expect(wd_a2a, wd.at[pl.ds(0, 3), wd_half, :])
    send(wd.at[:, wd_half, :], wd.at[:, wd_half, :], partner, wshare)
    up(3)
    h_start(3)
    expect(wshare, wd.at[:, wd_half, :])

    def down(k, group, at):
        size = 4 * at.size
        lhs = hid[group, :, at].reshape(size, FS)
        for j in range(4):
            part = jnp.dot(lhs, wd[j], preferred_element_type=F32).reshape(4, at.size, W)
            for kind in range(2):
                lanes = slice(kind * 128, kind * 128 + 128)
                pf[k, kind, j, :, at] = part[:, :, lanes]
                pb[k, kind, j, :, at] = part[:, :, lanes].astype(BF)

    class Reduce:
        def __init__(self, k, kind, at):
            self.k, self.kind, self.rows = k, kind, at
            self.pos, self.dev = ((y, at_y), (x, at_x))[kind]
            self.pos2, self.dev2 = ((x, at_x), (y, at_y))[kind]

        def item(self, to, first, count):
            where = (pl.ds(first, count), to) if self.kind == 0 else (to, pl.ds(first, count))
            return (self.k, self.kind, *where, self.rows)

        def of(self, ref, *where):
            return (ref.at[(self.k, self.kind, *where, self.rows)])

        def first(self):
            self.on_m, self.on_2 = channel(), channel()
            if self.k == 3:
                for d in (2, 1, 3):
                    part = pb.at[self.item(turn(self.pos, d), 0, 4)]
                    send(part, direct.at[self.kind, d - 1, :, self.rows], self.dev(d), self.on_m)
                return
            self.on_p = channel()
            far, p, m = turn(self.pos, 2), turn(self.pos, 1), turn(self.pos, -1)
            self.p, self.m = p, m
            low, high = pl.ds(0, 2), pl.ds(2, 2)
            self.op = send(pb.at[self.item(far, 0, 2)], self.of(opp_p, slice(None)), self.dev(1))
            self.om = send(pb.at[self.item(far, 2, 2)], self.of(opp_m, slice(None)), self.dev(-1))
            send(pb.at[self.item(p, 2, 2)], self.of(from_m, high), self.dev(1), self.on_m)
            send(pb.at[self.item(m, 0, 2)], self.of(from_p, low), self.dev(-1), self.on_p)

        def second(self):
            at = (self.k, self.kind)
            self.op.wait_recv()
            sum_p[at] = (pf[self.item(self.p, 0, 2)] + opp_p[at].astype(F32)).astype(BF)
            send(sum_p.at[at], self.of(from_m, pl.ds(0, 2)), self.dev(1), self.on_m)
            self.om.wait_recv()
            sum_m[at] = (pf[self.item(self.m, 2, 2)] + opp_m[at].astype(F32)).astype(BF)
            send(sum_m.at[at], self.of(from_p, pl.ds(2, 2)), self.dev(-1), self.on_p)

        def third(self):
            total = pf[self.item(self.pos, 0, 4)]
            if self.k == 3:
                expect(self.on_m, direct.at[self.kind, :, :, self.rows])
                for d in range(3):
                    total = total + direct[self.kind, d, :, self.rows].astype(F32)
            else:
                at = (self.k, self.kind)
                expect(self.on_m, from_m.at[at])
                expect(self.on_p, from_p.at[at])
                total = total + from_m[at].astype(F32) + from_p[at].astype(F32)
            rsum[self.k, self.kind, :, self.rows] = total
            tosend[self.k, self.kind, :, self.rows] = total.astype(BF)
            for d in (1, 3, 2):
                to = turn(self.pos2, d)
                send(self.of(tosend, to), self.of(torecv, d - 1), self.dev2(d), self.on_2)

        def fourth(self, group):
            expect(self.on_2, self.of(torecv, slice(None)))
            branch = rsum[self.k, self.kind, self.pos2, self.rows]
            for d in range(3):
                branch = branch + torecv[self.k, self.kind, d, self.rows].astype(F32)
            lanes = slice(self.kind * 128, self.kind * 128 + 128)
            mixed = residual_scale * nloc[group, self.rows, lanes].astype(F32) + branch
            mo[group, self.rows, lanes] = mixed
            mob[y, places[self.k], self.rows, lanes] = mixed.astype(BF)

    groups = [z, turn(z, -1), turn(z, 1), turn(z, 2)]
    places = [1, 0, 2, 3]
    batches = [(0, pl.ds(0, Q)), (1, pl.ds(0, Q)), (2, pl.ds(0, Q)), (3, pl.ds(0, 48)), (3, pl.ds(48, 48))]
    reduces = [(Reduce(k, 0, at), Reduce(k, 1, at)) for k, at in batches]

    def first(b):
        k, at = batches[b]
        down(k, groups[k], at)
        for one in reduces[b]:
            one.first()

    def second_(b):
        for one in reduces[b]:
            one.second()

    def third(b):
        for one in reduces[b]:
            one.third()

    def fourth(b):
        for one in reduces[b]:
            one.fourth(groups[batches[b][0]])

    def h_finish(late):
        expect(hon[late], hid.at[0, :, pl.ds(0, 48), :])

    first(0)
    h_forward(0, 0)
    h_forward(1, 0)
    second_(0)
    h_forward(2, 0)
    third(0)
    h_forward(3, 0)
    for n in range(4):
        h_forward(n, 1)
    def gather(place):
        def mblk(i, half):
            if half is None:
                return mob.at[i, place]
            return mob.at[i, place, pl.ds(half * 48, 48)]

        ring = Ring(y, at_y, mob.at[pl.ds(0, 2), 0], mblk)
        ring.start()
        return ring

    first(1)
    first(2)
    fourth(0)
    gathers = [gather(places[0])]
    second_(1)
    h_finish(0)
    first(3)
    second_(2)
    h_finish(1)
    first(4)
    third(1)
    gathers[0].forward()
    third(2)
    third(3)
    third(4)
    fourth(1)
    gathers.append(gather(places[1]))
    fourth(2)
    gathers.append(gather(places[2]))
    fourth(3)
    fourth(4)

    stat = exchange_start(tx_s, sums_of([mo[i] for i in range(4)]), tx_r, at_x, 4)
    last = channel()
    for d in (1, 3, 2):
        send(mob.at[y, 3], mob.at[y, 3], at_y(d), last)
    totals[0] = exchange_end(stat, tx_s, tx_r)
    stat = channel()
    pl.semaphore_wait(plane_y, 3)
    for d in range(1, 16):
        send(totals.at[0], totals.at[d], at_zy(d), stat)
    gathers[1].forward()
    gathers[2].forward()
    for ring in gathers:
        ring.finish()
    expect(last, mob.at[pl.ds(0, 3), 3])
    expect(stat, totals.at[pl.ds(1, 15)])
    columns = columns_of([totals[i] + totals[4 + i] + totals[8 + i] + totals[12 + i] for i in range(4)])
    for dy in range(4):
        yy = turn(y, -dy)
        for g in range(4):
            mean, scale = moments(columns, dy * 8 + g)
            block = (mob[yy, turn(1 - z, g)].astype(F32) - mean) * scale
            obuf[yy, g] = (block * go[...] + bo[...]).astype(BF)
            fetch(obuf.at[yy, g], out.at[g, yy], 4)
    assert len(used) == N_RECV, len(used)
    for copy in remote[-N_SEND:]:
        copy.wait_send()
    pltpu.make_async_copy(obuf, out, local_sem.at[4]).wait()


N_SEND = 48
N_RECV = 105
N_LOCAL = 5


def per_device(carried, branch_in, gain_in, bias_in, up_weight, down_weight, gain_out, bias_out):
    any_spec = pl.BlockSpec(memory_space=pl.ANY)
    vmem_spec = pl.BlockSpec(memory_space=pltpu.VMEM)
    V = pltpu.VMEM
    result = pl.pallas_call(
        kernel,
        out_shape=jax.ShapeDtypeStruct((4, 4, Q, W), BF),
        in_specs=[any_spec, any_spec, vmem_spec, vmem_spec, any_spec, any_spec, vmem_spec, vmem_spec],
        out_specs=any_spec,
        scratch_shapes=[
            V((4, Q, W), BF), V((4, Q, W), BF), V((4, Q, W), BF),
            V((G, D), BF), V((D, FS), BF), V((4, FS, W), BF), V((4, 4, Q, FS), BF),
            V((4, 2, 4, 4, Q, 128), F32), V((4, 2, 4, 4, Q, 128), BF),
            *[V((3, 2, 2, Q, 128), BF) for _ in range(4)],
            V((3, 2, 4, Q, 128), BF), V((3, 2, 4, Q, 128), BF), V((2, 3, 4, Q, 128), BF),
            V((4, 2, 4, Q, 128), F32), V((4, 2, 4, Q, 128), BF), V((4, 2, 3, Q, 128), BF),
            V((4, Q, W), F32), V((4, 4, Q, W), BF), V((4, 4, Q, W), BF),
            V((8, 128), F32), V((15, 8, 128), F32),
            V((8, 128), F32), V((3, 8, 128), F32), V((16, 8, 128), F32),
            pltpu.SemaphoreType.DMA((N_SEND,)),
            pltpu.SemaphoreType.DMA((N_RECV,)),
            pltpu.SemaphoreType.DMA((N_LOCAL,)),
            *[pltpu.SemaphoreType.REGULAR] * 3,
        ],
        compiler_params=pltpu.CompilerParams(
            collective_id=0, has_side_effects=True, vmem_limit_bytes=60 * 1024 * 1024
        ),
    )(
        carried.reshape(4, 4, Q, W), branch_in.reshape(4, 4, Q, W),
        gain_in.reshape(1, W), bias_in.reshape(1, W), up_weight, down_weight,
        gain_out.reshape(1, W), bias_out.reshape(1, W),
    )
    return result.reshape(carried.shape)


def solution(mesh):
    in_specs = (
        P("dp", "ra"),
        P("dp", "ra"),
        P("ra"),
        P("ra"),
        P("ra", "cb"),
        P("cb", "ra"),
        P("ra"),
        P("ra"),
    )
    out_specs = P("dp", "ra")
    return jax.shard_map(
        per_device, mesh=mesh, in_specs=in_specs, out_specs=out_specs, check_vma=False
    )
```
